32 devices in a mesh: fs: 4 (over y, x), tp: 8 (over z, core).
Axes of the slice: x: 2, y: 2, z: 4, core: 2. Of those that a mesh axis runs over, the one named last changes fastest.
Arguments:
- tokens: bfloat16 [4096, 2048], P(('fs', 'tp')), may hold values from -6 to 6
- up_gate: bfloat16 [4096, 5632], P('fs', 'tp'), may hold values from -8 to 8
- up_val: bfloat16 [4096, 5632], P('fs', 'tp'), may hold values from -6 to 6
- gate_weight: bfloat16 [2048, 5632], P('fs', 'tp'), may hold values from -0.125 to 0.125
- val_weight: bfloat16 [2048, 5632], P('fs', 'tp'), may hold values from -0.125 to 0.125
- gate_taps: bfloat16 [3, 5632], P(None, 'tp'), may hold values from -3 to 3
- val_taps: bfloat16 [3, 5632], P(None, 'tp'), may hold values from -3 to 3
- hidden_grad: bfloat16 [4096, 5632], P('fs', 'tp'), may hold values from -6 to 6
Outputs:
- input_grad: bfloat16 [4096, 2048], P(('fs', 'tp'))
- gate_weight_grad: float32 [2048, 5632], P('fs', 'tp')
- val_weight_grad: float32 [2048, 5632], P('fs', 'tp')
- gate_taps_grad: float32 [3, 5632], P(None, 'tp')
- val_taps_grad: float32 [3, 5632], P(None, 'tp')
- gate_row_norms: float32 [2048], P('fs')
- val_row_norms: float32 [2048], P('fs')
- tap_row_norms: float32 [2, 3], replicated
The draws below stay inside these ranges and needn't reach their ends.
All inputs are finite; a program needn't handle non-finite values.
Results may differ from the reference program's by a relative error of at most 0.017.
Values may be sent and summed in bfloat16 or wider, within the bound.
A program may use at most 128 MiB of HBM per device.

```python
import jax
import jax.numpy as jnp
from jax import lax

D = 2048
FF = 5632
TAPS = 3
SEQ = 1024
TOKENS = 4096
N_TP = 8


def spiked(entries, stream_key, source, target, parts, factor):
    owner, partner = [(jnp.arange(entries.shape[axis_at]) // (entries.shape[axis_at] // parts)).reshape([-1 if axis == axis_at else 1 for axis in range(entries.ndim)]) for axis_at in (source, target)]
    chosen = jax.random.permutation(stream_key, parts)[partner]
    strong = (owner == chosen) | (owner == (partner + parts // 2) % parts)
    return jnp.where(strong, factor * entries, entries)


def shard_levels(stream_key, dims, shards, smallest, top_value):
    def one(dim, parts):
        steps = jax.random.uniform(jax.random.fold_in(jax.random.fold_in(stream_key, 6), dim), (parts,), jnp.float32, smallest / len(shards), top_value / len(shards))
        return jnp.repeat(jnp.exp(steps), dims[dim] // parts).reshape((-1,) + (1,) * (len(dims) - dim - 1))

    factor_of = one(*shards[0])
    for cut in shards[1:]:
        factor_of = factor_of * one(*cut)
    return factor_of


def scatter_about(rng, shape, width, most, split=(), kind=jnp.bfloat16):
    entries = jax.random.normal(rng, shape, jnp.float32) * width
    if len(split) > 0:
        entries = shard_levels(rng, shape, split, -0.22, 0.18) * entries
    return jnp.clip(entries, min=-most, max=most).astype(kind)


def noise_with(own_key, shape, spread, most, pieces, heavy, kind=jnp.bfloat16):
    drawn = spread * jax.random.normal(own_key, shape, jnp.float32)
    if pieces:
        drawn = drawn * shard_levels(own_key, shape, pieces, -0.22, 0.18)
    return jnp.clip(spiked(drawn, jax.random.fold_in(own_key, 3), *heavy), -most, most).astype(kind)


def setup_inputs(seed: int = 0) -> dict:
    arg_keys = jax.random.split(jax.random.key(seed), 9)
    tokens = noise_with(arg_keys[0], (TOKENS, D), 1.0, 6.0, ((0, 32),), (0, 1, 32, 2.75))
    up_gate = scatter_about(arg_keys[1], (TOKENS, FF), 1.5, 8.0, ((0, 4), (1, 8)))
    up_val = scatter_about(arg_keys[2], (TOKENS, FF), 1.0, 6.0, ((0, 4), (1, 8)))
    gate_weight = scatter_about(arg_keys[3], (D, FF), D ** -0.5, 0.125, ((0, 4), (1, 8)))
    val_weight = scatter_about(arg_keys[4], (D, FF), D ** -0.5, 0.125, ((0, 4), (1, 8)))
    gate_taps = scatter_about(arg_keys[5], (TAPS, FF), 0.6, 3.0, ((1, 8),))
    val_taps = scatter_about(arg_keys[6], (TAPS, FF), 0.6, 3.0, ((1, 8),))
    hidden_grad = noise_with(arg_keys[7], (TOKENS, FF), 1.0, 6.0, ((0, 4), (1, 8)), (0, 1, 8, 2.0))
    return {"tokens": tokens, "up_gate": up_gate, "up_val": up_val, "gate_weight": gate_weight, "val_weight": val_weight, "gate_taps": gate_taps, "val_taps": val_taps, "hidden_grad": hidden_grad}


def shifted_sum(padded, kernel, length, backward):
    tap_count = kernel.shape[0]
    result = jnp.zeros((padded.shape[0], length, padded.shape[2]), jnp.float32)
    for tap_index in range(tap_count):
        tap_shift = tap_count - 1 - tap_index if backward else tap_index
        result = result + kernel[tap_index][None, None, :] * padded[:, tap_shift:tap_shift + length]
    return result


def local_grads(up_gate, up_val, hidden_grad, gate_taps, val_taps):
    length = up_gate.shape[1]
    tap_count = gate_taps.shape[0]
    gate_kernel = gate_taps.astype(jnp.float32)
    val_kernel = val_taps.astype(jnp.float32)
    pad_front = ((0, 0), (tap_count - 1, 0), (0, 0))
    pad_back = ((0, 0), (0, tap_count - 1), (0, 0))
    padded_gate = jnp.pad(up_gate.astype(jnp.float32), pad_front)
    padded_val = jnp.pad(up_val.astype(jnp.float32), pad_front)
    conv_gate = shifted_sum(padded_gate, gate_kernel, length, False)
    conv_val = shifted_sum(padded_val, val_kernel, length, False)
    sigmoid_gate = jax.nn.sigmoid(conv_gate)
    grad_hidden = hidden_grad.astype(jnp.float32)
    val_back = grad_hidden * conv_gate * sigmoid_gate
    gate_back = grad_hidden * conv_val * sigmoid_gate * (1.0 + conv_gate * (1.0 - sigmoid_gate))
    up_gate_back = shifted_sum(jnp.pad(gate_back, pad_back), gate_kernel, length, True).astype(jnp.bfloat16)
    up_val_back = shifted_sum(jnp.pad(val_back, pad_back), val_kernel, length, True).astype(jnp.bfloat16)
    tap_gate = jnp.stack([jnp.sum(padded_gate[:, tap_index:tap_index + length] * gate_back, axis=(0, 1))
                          for tap_index in range(tap_count)])
    tap_val = jnp.stack([jnp.sum(padded_val[:, tap_index:tap_index + length] * val_back, axis=(0, 1))
                         for tap_index in range(tap_count)])
    return up_gate_back, up_val_back, tap_gate, tap_val


def reference(tokens, up_gate, up_val, gate_weight, val_weight, gate_taps, val_taps, hidden_grad):
    width_in = tokens.shape[1]
    hidden_units = up_gate.shape[1]
    block_width = hidden_units // N_TP
    seq_count = tokens.shape[0] // SEQ
    gate_float = gate_weight.astype(jnp.float32).reshape(width_in, N_TP, block_width)
    val_float = val_weight.astype(jnp.float32).reshape(width_in, N_TP, block_width)

    def slice_rows(values, row_start):
        return lax.dynamic_slice_in_dim(values, row_start, SEQ, 0)

    def one_sequence(totals, seq_index):
        row_start = (seq_index * SEQ).astype(jnp.int32)
        local_back = local_grads(slice_rows(up_gate, row_start)[None], slice_rows(up_val, row_start)[None],
                                 slice_rows(hidden_grad, row_start)[None], gate_taps, val_taps)
        gate_back = local_back[0][0]
        val_back = local_back[1][0]
        rows_in = slice_rows(tokens, row_start)
        gate_total = totals[0] + jnp.dot(rows_in.T, gate_back, preferred_element_type=jnp.float32)
        val_total = totals[1] + jnp.dot(rows_in.T, val_back, preferred_element_type=jnp.float32)
        tap_gate_total = totals[2] + local_back[2]
        tap_val_total = totals[3] + local_back[3]
        partials = jnp.einsum('sjf,djf->jsd', gate_back.astype(jnp.float32).reshape(SEQ, N_TP, block_width), gate_float)
        partials = partials + jnp.einsum('sjf,djf->jsd', val_back.astype(jnp.float32).reshape(SEQ, N_TP, block_width), val_float)
        rounded = lax.optimization_barrier(partials.astype(jnp.bfloat16))
        input_rows = jnp.sum(rounded.astype(jnp.float32), axis=0).astype(jnp.bfloat16)
        return (gate_total, val_total, tap_gate_total, tap_val_total), input_rows

    tap_count = gate_taps.shape[0]
    init = (jnp.zeros((width_in, hidden_units), jnp.float32), jnp.zeros((width_in, hidden_units), jnp.float32),
            jnp.zeros((tap_count, hidden_units), jnp.float32), jnp.zeros((tap_count, hidden_units), jnp.float32))
    totals, input_rows = lax.scan(one_sequence, init, jnp.arange(seq_count, dtype=jnp.int32))
    gate_grad, val_grad, tap_gate, tap_val = totals
    input_grad = input_rows.reshape(tokens.shape)
    gate_norms = jnp.sum(gate_grad * gate_grad, axis=1)
    val_norms = jnp.sum(val_grad * val_grad, axis=1)
    tap_norms = jnp.stack([jnp.sum(tap_gate * tap_gate, axis=1), jnp.sum(tap_val * tap_val, axis=1)])
    return (input_grad, gate_grad, val_grad, tap_gate, tap_val, gate_norms, val_norms, tap_norms)
```

```python
import functools

import jax
import jax.numpy as jnp
from jax import lax
from jax.experimental import pallas as pl
from jax.experimental.pallas import tpu as pltpu
from jax.sharding import PartitionSpec as P

SEQ = 1024
CORES = 2
MESH = pl.DeviceIdType.MESH
ANY = pl.BlockSpec(memory_space=pl.ANY)
VMEM = pl.BlockSpec(memory_space=pltpu.VMEM)


def hidden_chunks(hidden):
    if hidden % 64:
        return [(0, hidden)]
    sizes = [128] * (hidden // 128) + ([64] if hidden % 128 else [])
    chunks, at = [], 0
    for size in sizes:
        chunks.append((at, size))
        at += size
    return chunks


def piece_shifts(chips):
    return sorted(range(1, chips), key=lambda s: (-min(s, chips - s), s)) + [0]


def stream_steps(n, pieces):
    steps, ready = [], []
    lead = max(0, n - pieces)
    for k in range(lead):
        steps.append((k, k + 1, None))
        ready.append(("chunk", k, len(steps)))
    for j in range(pieces):
        steps.append((lead, n, j))
        if j == pieces - 1:
            for k in range(lead, n):
                ready.append(("chunk", k, len(steps)))
        ready.append(("piece", j, len(steps)))
        if j < pieces - 1 and lead < n - 1:
            for rest in range(j + 1, pieces):
                steps.append((lead, lead + 1, rest))
            ready.append(("chunk", lead, len(steps)))
            lead += 1
    return steps, ready


def conv_rows(group, rows, taps, at, base, size, gate_ref, val_ref, grad_ref, kern_ref, back_ref, tap_ref):
    place = lax.broadcasted_iota(jnp.int32, (group, rows), 1) % SEQ
    lane = lax.broadcasted_iota(jnp.int32, (group, 128), 1)

    def one(index, carry):
        here = pl.multiple_of(at + index * group, group)
        src = pl.ds(here, group)
        kernels = kern_ref[src, :]
        gate_kernel = kernels[:, 0:taps]
        val_kernel = kernels[:, taps : 2 * taps]

        def delayed(field, shift):
            if shift == 0:
                return field
            return jnp.where(place >= shift, pltpu.roll(field, shift, 1), 0.0)

        def advanced(field, shift):
            if shift == 0:
                return field
            return jnp.where(place < SEQ - shift, pltpu.roll(field, rows - shift, 1), 0.0)

        def mixed(fields, kernel):
            total = fields[0] * kernel[:, 0:1]
            for i in range(1, taps):
                total = total + fields[i] * kernel[:, i : i + 1]
            return total

        gate = gate_ref[src, :].astype(jnp.float32)
        val = val_ref[src, :].astype(jnp.float32)
        gate_fields = [delayed(gate, taps - 1 - i) for i in range(taps)]
        val_fields = [delayed(val, taps - 1 - i) for i in range(taps)]
        conv_gate = mixed(gate_fields, gate_kernel)
        conv_val = mixed(val_fields, val_kernel)
        sigmoid = jax.nn.sigmoid(conv_gate)
        scaled = grad_ref[src, :].astype(jnp.float32) * sigmoid
        val_back = scaled * conv_gate
        gate_back = scaled * conv_val * (1.0 + conv_gate * (1.0 - sigmoid))
        row = pl.multiple_of(base + index * group, group)
        back_ref[0, pl.ds(row, group), :] = mixed(
            [advanced(gate_back, taps - 1 - i) for i in range(taps)], gate_kernel
        ).astype(jnp.bfloat16)
        row = pl.multiple_of(base + size + index * group, group)
        back_ref[0, pl.ds(row, group), :] = mixed(
            [advanced(val_back, taps - 1 - i) for i in range(taps)], val_kernel
        ).astype(jnp.bfloat16)
        sums = jnp.zeros((group, 128), jnp.float32)
        for i in range(taps):
            sums = jnp.where(lane == i, jnp.sum(gate_fields[i] * gate_back, axis=1, keepdims=True), sums)
            sums = jnp.where(
                lane == taps + i, jnp.sum(val_fields[i] * val_back, axis=1, keepdims=True), sums
            )
        tap_ref[src, :] = sums
        return carry

    lax.fori_loop(0, size // group, one, 0)


def step_kernel(
    fa, fb, chips, taps,
    tok_ref, up_gate_ref, up_val_ref, gw_ref, vw_ref, kern_ref, grad_ref,
    dx_ref, gate_out, val_out, tap_out, norm_out,
    fg, fv, fh, tok, back, wg, wv, wt, pown, psend, precv, ssend, zrecv, xsend, xrecv,
    gsend, grecv, tapbuf, tapx, normx,
    load_sem, tokx_s, tokx_r, tokz_s, tokz_r, relay_s, tokc_s, tokc_r, w_s, w_r,
    back_s, back_r, pc_s, pc_r, pz_s, pz_r, out_s, out_r, g_s, g_r, tap_s, tap_r, norm_s, norm_r,
):
    f32, bf16 = jnp.float32, jnp.bfloat16
    fs_at = lax.axis_index("fs")
    tp_at = lax.axis_index("tp")
    a_at, b_at = fs_at // fb, fs_at % fb
    z_at, c_at = tp_at // CORES, tp_at % CORES
    hidden, rows = up_gate_ref.shape
    shard, width = tok_ref.shape
    block = gw_ref.shape[1]
    wide = fa * block
    piece = CORES * shard
    chunks = hidden_chunks(hidden)
    shifts = piece_shifts(chips)
    steps, ready = stream_steps(len(chunks), chips)
    tp_size = chips * CORES
    fs_size = fa * fb

    def x_peer(d):
        return (a_at * fb + (b_at + d) % fb, tp_at)

    def y_peer(d):
        return (((a_at + d) % fa) * fb + b_at, tp_at)

    def z_peer(z):
        return (fs_at, z * CORES + c_at)

    core_peer = (fs_at, z_at * CORES + (CORES - 1 - c_at))

    def remote(src, dst, send, recv, peer):
        return pltpu.make_async_remote_copy(
            src_ref=src, dst_ref=dst, send_sem=send, recv_sem=recv, device_id=peer, device_id_type=MESH
        )

    loads = []

    def load(src, dst):
        copy = pltpu.make_async_copy(src, dst, load_sem.at[len(loads)])
        copy.start()
        loads.append(copy)
        return copy

    field_loads = []
    for at, size in chunks:
        cut = pl.ds(at, size)
        field_loads.append(
            [load(s.at[cut], d.at[cut]) for s, d in ((up_gate_ref, fg), (up_val_ref, fv), (grad_ref, fh))]
        )

    def token_columns(d, d_a):
        start = (((a_at + d_a) % fa) * fb + (b_at + d) % fb) * block
        return tok_ref.at[:, pl.ds(pl.multiple_of(start, block), block)]

    def token_rows(z, c):
        return pl.ds(pl.multiple_of((z * CORES + c) * shard, shard), shard)

    mine = token_rows(z_at, c_at)
    tok_loads = [
        load(token_columns(0, d_a), tok.at[0, mine, pl.ds(d_a * block, block)]) for d_a in range(fa)
    ]
    w_loads = [load(gw_ref, wg.at[0]), load(vw_ref, wv.at[0])]

    barrier = pltpu.get_barrier_semaphore()
    peers = [((fs_at + d) % fs_size, tp_at) for d in range(1, fs_size)]
    peers += [(fs_at, (tp_at + d) % tp_size) for d in range(1, tp_size)]
    for peer in peers:
        pl.semaphore_signal(barrier, inc=1, device_id=peer, device_id_type=MESH)
    pl.semaphore_wait(barrier, len(peers))

    sends = []

    def send(copy):
        copy.start()
        sends.append(copy)
        return copy

    tokx = {}
    for d in range(1, fb):
        for d_a in range(fa):
            send(remote(
                token_columns(d, d_a), tok.at[fb - d, mine, pl.ds(d_a * block, block)],
                tokx_s.at[d - 1, d_a], tokx_r.at[fb - d - 1, d_a], x_peer(d),
            ))
            tokx[fb - d, d_a] = sends[-1]
    w_waits = {}
    for d in range(1, fa):
        for i, (src, dst) in enumerate(((gw_ref, wg), (vw_ref, wv))):
            send(remote(src, dst.at[fa - d], w_s.at[d - 1, i], w_r.at[fa - d - 1, i], y_peer(d)))
            w_waits[fa - d, i] = remote(
                src, dst.at[fa - d], w_s.at[d - 1, i], w_r.at[fa - d - 1, i], y_peer(d)
            )

    late = []

    def distance(u, v):
        return jnp.abs(u - v)

    def tok_z(s):
        for j in range(1, chips):
            to = (z_at + j) % chips

            copy = remote(
                tok.at[s, mine], tok.at[s, mine], tokz_s.at[s, j - 1], tokz_r.at[s, z_at], z_peer(to)
            )
            direct = distance(to, z_at) != 2

            @pl.when(direct)
            def _(copy=copy):
                copy.start()

            late.append((direct, copy))
        send(remote(tok.at[s, mine], tok.at[s, mine], tokc_s.at[s, z_at], tokc_r.at[s, z_at], core_peer))

    def tok_arrived(s, source):
        at = token_rows(source, c_at)
        remote(tok.at[s, at], tok.at[s, at], tokz_s.at[s, 0], tokz_r.at[s, source], z_peer(z_at)).wait_recv()

    def to_core(s, source):
        at = token_rows(source, c_at)
        send(remote(tok.at[s, at], tok.at[s, at], tokc_s.at[s, source], tokc_r.at[s, source], core_peer))

    def tok_relay(s):
        for side, step in enumerate((1, -1)):
            source, target = z_at - step, z_at + step
            exists = jnp.logical_and(source >= 0, source < chips)
            both = jnp.logical_and(exists, jnp.logical_and(target >= 0, target < chips))
            source = (source + chips) % chips
            target = (target + chips) % chips
            at = token_rows(source, c_at)
            copy = remote(
                tok.at[s, at], tok.at[s, at], relay_s.at[s, side], tokz_r.at[s, source], z_peer(target)
            )

            @pl.when(exists)
            def _(source=source):
                tok_arrived(s, source)

            @pl.when(both)
            def _(copy=copy):
                copy.start()

            late.append((both, copy))

            forward = remote(
                tok.at[s, at], tok.at[s, at], tokc_s.at[s, source], tokc_r.at[s, source], core_peer
            )

            @pl.when(exists)
            def _(forward=forward):
                forward.start()

            late.append((exists, forward))

    def tok_rest(s):
        for j in range(1, chips):
            source = (z_at + j) % chips
            far = distance(source, z_at) > 1
            at = token_rows(source, c_at)
            forward = remote(
                tok.at[s, at], tok.at[s, at], tokc_s.at[s, source], tokc_r.at[s, source], core_peer
            )

            @pl.when(far)
            def _(source=source, forward=forward):
                tok_arrived(s, source)
                forward.start()

            late.append((far, forward))

    def tok_from_core(s):
        for z in range(chips):
            at = token_rows(z, CORES - 1 - c_at)
            remote(tok.at[s, at], tok.at[s, at], tokc_s.at[s, z], tokc_r.at[s, z], core_peer).wait_recv()

    def lanes(j):
        return pl.ds(pl.multiple_of(((z_at + shifts[j]) % chips) * piece, piece), piece)

    def back_slice(slot, step):
        lo, hi, j = steps[step]
        first = 2 * chunks[lo][0]
        last = 2 * (chunks[hi - 1][0] + chunks[hi - 1][1])
        if j is None:
            return back.at[slot, pl.ds(first, last - first)]
        return back.at[slot, pl.ds(first, last - first), lanes(j)]

    back_waits = {}

    def send_back(step):
        for d in range(1, fb):
            send(remote(
                back_slice(0, step), back_slice(fb - d, step),
                back_s.at[d - 1, step], back_r.at[fb - d - 1, step], x_peer(d),
            ))

    got = [0]

    def await_back(until):
        while got[0] < until:
            step = got[0]
            for s in range(1, fb):
                remote(
                    back_slice(0, step), back_slice(s, step),
                    back_s.at[0, step], back_r.at[s - 1, step], x_peer(1 % fb),
                ).wait_recv()
            got[0] += 1

    if tapbuf.shape[0] > hidden:
        tapbuf[hidden:, :] = jnp.zeros((tapbuf.shape[0] - hidden, 128), f32)

    for copy in tok_loads:
        copy.wait()
    tok_z(0)
    next_step = 0
    after_conv = {0: [lambda: [tok_x_done(), [tok_z(s) for s in range(1, fb)]]]}

    def tok_x_done():
        for s in range(1, fb):
            for d_a in range(fa):
                tokx[s, d_a].wait_recv()

    relays = list(range(fb))
    for k, (at, size) in enumerate(chunks):
        for copy in field_loads[k]:
            copy.wait()
        group = 16 if size % 16 == 0 else 8
        conv_rows(group, rows, taps, at, 2 * at, size, fg, fv, fh, kern_ref, back, tapbuf)
        while next_step < len(steps) and steps[next_step][1] <= k + 1:
            send_back(next_step)
            next_step += 1
        for action in after_conv.get(k, []):
            action()
        if k >= 1 and k % 2 == 0 and relays and k < len(chunks) - 1:
            tok_relay(relays.pop(0))

    tap_t = tapbuf[...].T
    tapx[fs_at] = tap_t[0 : tapx.shape[1], :]
    for d in range(1, fs_size):
        to = ((fs_at + d) % fs_size, tp_at)
        send(remote(tapx.at[fs_at], tapx.at[fs_at], tap_s.at[d - 1], tap_r.at[fs_at], to))

    while relays:
        tok_relay(relays.pop(0))

    def transpose_weights(d):
        for at, size in chunks:
            pair = jnp.concatenate((wg[d, pl.ds(at, size), :], wv[d, pl.ds(at, size), :]), axis=0)
            wt[pl.ds(d * block, block), pl.ds(2 * at, 2 * size)] = pair.T

    for copy in w_loads:
        copy.wait()
    transpose_weights(0)
    for d in range(1, fa):
        for i in range(2):
            w_waits[d, i].wait_recv()
        transpose_weights(d)

    inner = (((1,), (0,)), ((), ()))
    mblock = min(256, wide)

    def partial(r, j):
        right = back[r, :, lanes(j)]

        def one(i, carry):
            at = pl.ds(pl.multiple_of(i * mblock, mblock), mblock)
            out = lax.dot_general(wt[at, :], right, inner, preferred_element_type=f32).astype(bf16)
            own = jnp.where(c_at == 0, out[:, 0:shard], out[:, shard:piece])
            other = jnp.where(c_at == 0, out[:, shard:piece], out[:, 0:shard])
            pown[r, j, at, :] = own
            psend[r, j, at, :] = other
            return carry

        lax.fori_loop(0, wide // mblock, one, 0)
        send(remote(psend.at[r, j], precv.at[r, j], pc_s.at[r, j], pc_r.at[r, j], core_peer))

    def reduce_core(r, j):
        remote(psend.at[r, j], precv.at[r, j], pc_s.at[r, j], pc_r.at[r, j], core_peer).wait_recv()
        total = pown[r, j].astype(f32) + precv[r, j].astype(f32)
        ssend[r, j] = total.astype(bf16)
        if shifts[j]:
            to = (z_at + shifts[j]) % chips
            send(remote(ssend.at[r, j], zrecv.at[r, j], pz_s.at[r, j], pz_r.at[r, j], z_peer(to)))

    def reduce_chips(r):
        total = ssend[r, chips - 1].astype(f32)
        for j in range(chips - 1):
            remote(ssend.at[r, j], zrecv.at[r, j], pz_s.at[r, j], pz_r.at[r, j], z_peer(z_at)).wait_recv()
            total = total + zrecv[r, j].astype(f32)
        return total.astype(bf16).T

    def gradient(k):
        at, size = chunks[k]
        cut = pl.ds(2 * at, 2 * size)
        for d_a in list(range(1, fa)) + [0]:
            cols = slice(d_a * block, (d_a + 1) * block)
            total = lax.dot_general(back[0, cut, :], tok[0, :, cols], inner, preferred_element_type=f32)
            for s in range(1, fb):
                total = total + lax.dot_general(
                    back[s, cut, :], tok[s, :, cols], inner, preferred_element_type=f32
                )
            if d_a:
                gsend[d_a - 1, cut, :] = total.astype(bf16)
                send(remote(
                    gsend.at[d_a - 1, cut], grecv.at[fa - d_a - 1, cut],
                    g_s.at[d_a - 1, k], g_r.at[fa - d_a - 1, k], y_peer(d_a),
                ))
            else:
                gate_out[pl.ds(at, size), :] = total[:size]
                val_out[pl.ds(at, size), :] = total[size:]

    def finish_gradient(k, norms):
        at, size = chunks[k]
        cut = pl.ds(2 * at, 2 * size)
        for s in range(1, fa):
            remote(
                gsend.at[s - 1, cut], grecv.at[s - 1, cut], g_s.at[s - 1, k], g_r.at[s - 1, k], y_peer(1 % fa)
            ).wait_recv()
        new = []
        for i, out in enumerate((gate_out, val_out)):
            rows_at = pl.ds(at, size)
            total = out[rows_at, :]
            for s in range(1, fa):
                total = total + grecv[s - 1, pl.ds(2 * at + i * size, size), :].astype(f32)
            out[rows_at, :] = total
            new.append(norms[i] + jnp.sum(total * total, axis=0, keepdims=True))
        return new

    for j in range(chips):
        partial(0, j)
        if j:
            reduce_core(0, j - 1)
    for s in range(fb):
        tok_rest(s)
    reduce_core(0, chips - 1)
    for s in range(fb):
        tok_from_core(s)

    waiting = []
    for kind, index, until in ready:
        await_back(until)
        if kind == "chunk":
            gradient(index)
            for r, j in waiting:
                reduce_core(r, j)
            waiting = []
        else:
            for r, j in waiting:
                reduce_core(r, j)
            waiting = []
            for r in range(1, fb):
                partial(r, index)
                waiting.append((r, index))

    def place(slot, value):
        for d_a in range(fa):
            start = (((a_at + d_a) % fa) * fb + (b_at + slot) % fb) * block
            dx_ref[:, pl.ds(pl.multiple_of(start, block), block)] = value[:, d_a * block : (d_a + 1) * block]

    place(0, reduce_chips(0))
    for r, j in waiting:
        reduce_core(r, j)

    tap_total = None
    for f in range(fs_size):
        @pl.when(fs_at != f)
        def _(f=f):
            remote(tapx.at[f], tapx.at[f], tap_s.at[0], tap_r.at[f], (fs_at, tp_at)).wait_recv()

        tap_total = tapx[f] if f == 0 else tap_total + tapx[f]
    tap_out[...] = tap_total
    tap_norms = jnp.sum(tap_total * tap_total, axis=1, keepdims=True)

    norms = [jnp.zeros((1, block), f32), jnp.zeros((1, block), f32)]
    n = len(chunks)
    for k in range(max(0, n - 2)):
        norms = finish_gradient(k, norms)

    for r in range(1, fb):
        xsend[r - 1] = reduce_chips(r)
        send(remote(xsend.at[r - 1], xrecv.at[fb - r - 1], out_s.at[r - 1], out_r.at[fb - r - 1], x_peer(r)))

    for k in range(max(0, n - 2), n):
        norms = finish_gradient(k, norms)
    normx[tp_at, 0:1, :] = norms[0]
    normx[tp_at, 1:2, :] = norms[1]
    normx[tp_at, 2 : 2 + 2 * taps, :] = jnp.broadcast_to(tap_norms[0 : 2 * taps], (2 * taps, block))
    for d in range(1, tp_size):
        to = (fs_at, (tp_at + d) % tp_size)
        send(remote(normx.at[tp_at], normx.at[tp_at], norm_s.at[d - 1], norm_r.at[tp_at], to))

    for s in range(1, fb):
        remote(xsend.at[s - 1], xrecv.at[s - 1], out_s.at[s - 1], out_r.at[s - 1], x_peer(1 % fb)).wait_recv()
        place(s, xrecv[s - 1])

    norm_total = None
    for t in range(tp_size):
        @pl.when(tp_at != t)
        def _(t=t):
            remote(normx.at[t], normx.at[t], norm_s.at[0], norm_r.at[t], (fs_at, tp_at)).wait_recv()

        norm_total = normx[t] if t == 0 else norm_total + normx[t]
    norm_out[...] = norm_total

    for copy in sends:
        copy.wait_send()
    for held, copy in late:
        @pl.when(held)
        def _(copy=copy):
            copy.wait_send()


def whole_step(fa, fb, chips, taps, tokens, up_gate, up_val, gate_weight, val_weight, kernels, hidden_grad):
    f32, bf16 = jnp.float32, jnp.bfloat16
    hidden, rows = up_gate.shape
    shard, width = tokens.shape
    block = gate_weight.shape[1]
    wide = fa * block
    fs_size, tp_size = fa * fb, chips * CORES
    chunks = hidden_chunks(hidden)
    n = len(chunks)
    steps, _ = stream_steps(n, chips)
    padded = -(-hidden // 128) * 128
    tap_rows = -(-2 * taps // 8) * 8
    norm_rows = -(-(2 + 2 * taps) // 8) * 8
    dma = pltpu.SemaphoreType.DMA
    xs, ys = max(1, fb - 1), max(1, fa - 1)
    scratch = [
        pltpu.VMEM((hidden, rows), bf16),
        pltpu.VMEM((hidden, rows), bf16),
        pltpu.VMEM((hidden, rows), bf16),
        pltpu.VMEM((fb, rows, wide), bf16),
        pltpu.VMEM((fb, 2 * hidden, rows), bf16),
        pltpu.VMEM((fa, hidden, block), bf16),
        pltpu.VMEM((fa, hidden, block), bf16),
        pltpu.VMEM((wide, 2 * hidden), bf16),
        pltpu.VMEM((fb, chips, wide, shard), bf16),
        pltpu.VMEM((fb, chips, wide, shard), bf16),
        pltpu.VMEM((fb, chips, wide, shard), bf16),
        pltpu.VMEM((fb, chips, wide, shard), bf16),
        pltpu.VMEM((fb, chips, wide, shard), bf16),
        pltpu.VMEM((xs, shard, wide), bf16),
        pltpu.VMEM((xs, shard, wide), bf16),
        pltpu.VMEM((ys, 2 * hidden, block), bf16),
        pltpu.VMEM((ys, 2 * hidden, block), bf16),
        pltpu.VMEM((padded, 128), f32),
        pltpu.VMEM((fs_size, tap_rows, padded), f32),
        pltpu.VMEM((tp_size, norm_rows, block), f32),
        dma((3 * n + fa + 2,)),
        dma((xs, fa)),
        dma((xs, fa)),
        dma((fb, max(1, chips - 1))),
        dma((fb, chips)),
        dma((fb, 2)),
        dma((fb, chips)),
        dma((fb, chips)),
        dma((ys, 2)),
        dma((ys, 2)),
        dma((xs, len(steps))),
        dma((xs, len(steps))),
        dma((fb, chips)),
        dma((fb, chips)),
        dma((fb, chips)),
        dma((fb, chips)),
        dma((xs,)),
        dma((xs,)),
        dma((ys, n)),
        dma((ys, n)),
        dma((max(1, fs_size - 1),)),
        dma((fs_size,)),
        dma((max(1, tp_size - 1),)),
        dma((tp_size,)),
    ]
    return pl.pallas_call(
        functools.partial(step_kernel, fa, fb, chips, taps),
        in_specs=[ANY, ANY, ANY, ANY, ANY, VMEM, ANY],
        out_specs=[VMEM] * 5,
        out_shape=[
            jax.ShapeDtypeStruct((shard, width), bf16),
            jax.ShapeDtypeStruct((hidden, block), f32),
            jax.ShapeDtypeStruct((hidden, block), f32),
            jax.ShapeDtypeStruct((tap_rows, padded), f32),
            jax.ShapeDtypeStruct((norm_rows, block), f32),
        ],
        scratch_shapes=scratch,
        compiler_params=pltpu.CompilerParams(
            collective_id=0, has_side_effects=True, vmem_limit_bytes=60 * 1024 * 1024
        ),
    )(tokens, up_gate, up_val, gate_weight, val_weight, kernels, hidden_grad)


def solution(mesh):
    fs_size, tp_size = mesh.shape["fs"], mesh.shape["tp"]
    fb = max(d for d in range(1, fs_size + 1) if fs_size % d == 0 and d * d <= fs_size)
    fa = fs_size // fb
    chips = tp_size // CORES

    def local(tokens, up_gate, up_val, gate_weight, val_weight, gate_taps, val_taps, hidden_grad):
        taps, hidden = gate_taps.shape
        kernels = jnp.concatenate((gate_taps, val_taps), axis=0).astype(jnp.float32).T
        dx, gate_grad, val_grad, tap_grad, norms = whole_step(
            fa, fb, chips, taps, tokens, up_gate.T, up_val.T, gate_weight.T, val_weight.T,
            kernels, hidden_grad.T,
        )
        return (
            dx,
            gate_grad.T,
            val_grad.T,
            tap_grad[:taps, :hidden],
            tap_grad[taps : 2 * taps, :hidden],
            norms[0],
            norms[1],
            norms[2 : 2 + 2 * taps, 0].reshape(2, taps),
        )

    in_specs = (
        P(("fs", "tp"), None),
        P("fs", "tp"),
        P("fs", "tp"),
        P("fs", "tp"),
        P("fs", "tp"),
        P(None, "tp"),
        P(None, "tp"),
        P("fs", "tp"),
    )
    out_specs = (
        P(("fs", "tp"), None),
        P("fs", "tp"),
        P("fs", "tp"),
        P(None, "tp"),
        P(None, "tp"),
        P("fs"),
        P("fs"),
        P(),
    )
    return jax.shard_map(local, mesh=mesh, in_specs=in_specs, out_specs=out_specs, check_vma=False)
```

```python
import functools

import jax
import jax.numpy as jnp
from jax import lax
from jax.experimental import pallas as pl
from jax.experimental.pallas import tpu as pltpu
from jax.sharding import PartitionSpec as P

SEQ = 1024
CORES = 2
VMEM_LIMIT = 60 * 1024 * 1024
MESH = pl.DeviceIdType.MESH
ANY = pl.BlockSpec(memory_space=pl.ANY)
HBM = pl.BlockSpec(memory_space=pltpu.HBM)
VMEM = pl.BlockSpec(memory_space=pltpu.VMEM)


def hidden_chunks(hidden):
    if hidden % 64:
        return [(0, hidden)]
    units = hidden // 64
    small = min(5, units)
    small += (units - small) % 2
    sizes = [128] * ((units - small) // 2) + [64] * small
    chunks, at = [], 0
    for size in sizes:
        chunks.append((at, size))
        at += size
    return chunks


def piece_shifts(chips):
    return sorted(range(1, chips), key=lambda s: (-min(s, chips - s), s)) + [0]


def stream_steps(n, pieces):
    steps, ready = [], []
    heads = n - min(3, n)
    lead = max(0, min(2, heads - 1))

    def rest(k, j):
        for later in range(j + 1, pieces):
            steps.append((k, k + 1, later))
        ready.append(("chunk", k, len(steps)))

    for k in range(lead):
        steps.append((k, k + 1, None))
        ready.append(("chunk", k, len(steps)))
    for j in range(pieces - 1):
        steps.append((lead, n, j))
        ready.append(("piece", j, len(steps)))
        last = lead + 1 if j < pieces - 3 else heads
        while j < pieces - 2 and lead < min(last, heads):
            rest(lead, j)
            lead += 1
    for k in range(lead, n):
        steps.append((k, k + 1, pieces - 1))
        ready.append(("chunk", k, len(steps)))
    ready.append(("piece", pieces - 1, len(steps)))
    return steps, ready


def conv_rows(group, rows, taps, at, base, size, gate_ref, val_ref, grad_ref, kern_ref, back_ref, tap_ref):
    place = lax.broadcasted_iota(jnp.int32, (group, rows), 1) % SEQ
    lane = lax.broadcasted_iota(jnp.int32, (group, 128), 1)

    def one(index, carry):
        here = pl.multiple_of(at + index * group, group)
        src = pl.ds(here, group)
        kernels = kern_ref[src, :]
        gate_kernel = kernels[:, 0:taps]
        val_kernel = kernels[:, taps : 2 * taps]

        def delayed(field, shift):
            if shift == 0:
                return field
            return jnp.where(place >= shift, pltpu.roll(field, shift, 1), 0.0)

        def advanced(field, shift):
            if shift == 0:
                return field
            return jnp.where(place < SEQ - shift, pltpu.roll(field, rows - shift, 1), 0.0)

        def mixed(fields, kernel):
            total = fields[0] * kernel[:, 0:1]
            for i in range(1, taps):
                total = total + fields[i] * kernel[:, i : i + 1]
            return total

        gate = gate_ref[src, :].astype(jnp.float32)
        val = val_ref[src, :].astype(jnp.float32)
        gate_fields = [delayed(gate, taps - 1 - i) for i in range(taps)]
        val_fields = [delayed(val, taps - 1 - i) for i in range(taps)]
        conv_gate = mixed(gate_fields, gate_kernel)
        conv_val = mixed(val_fields, val_kernel)
        sigmoid = jax.nn.sigmoid(conv_gate)
        scaled = grad_ref[src, :].astype(jnp.float32) * sigmoid
        val_back = scaled * conv_gate
        gate_back = scaled * conv_val * (1.0 + conv_gate * (1.0 - sigmoid))
        row = pl.multiple_of(base + index * group, group)
        back_ref[0, pl.ds(row, group), :] = mixed(
            [advanced(gate_back, taps - 1 - i) for i in range(taps)], gate_kernel
        ).astype(jnp.bfloat16)
        row = pl.multiple_of(base + size + index * group, group)
        back_ref[0, pl.ds(row, group), :] = mixed(
            [advanced(val_back, taps - 1 - i) for i in range(taps)], val_kernel
        ).astype(jnp.bfloat16)
        sums = jnp.zeros((group, 128), jnp.float32)
        for i in range(taps):
            sums = jnp.where(lane == i, jnp.sum(gate_fields[i] * gate_back, axis=1, keepdims=True), sums)
            sums = jnp.where(
                lane == taps + i, jnp.sum(val_fields[i] * val_back, axis=1, keepdims=True), sums
            )
        tap_ref[src, :] = sums
        return carry

    lax.fori_loop(0, size // group, one, 0)


def step_kernel(
    fa, fb, chips, taps,
    tok_ref, up_gate_ref, up_val_ref, gw_ref, vw_ref, gate_taps_ref, val_taps_ref, grad_ref,
    dx_out, gate_done, val_done, tap_out, norm_out,
    fg, fv, fh, tok, back, wg, wv, wt, pown, psend, precv, ssend, zrecv, xsend, xrecv,
    gsend, grecv, tapbuf, tapx, normx, relayed, gtaps, vtaps, kern_in, kern_ref, dx_ref, gate_out, val_out, held, tap_held, norm_held,
    load_sem, tokx_s, tokx_r, tokz_s, tokz_r, relay_s, tokc_s, tokc_r, w_s, w_r,
    back_s, back_r, pc_s, pc_r, pz_s, pz_r, mid_r, out_s, out_r, g_s, g_r, tap_s, tap_r, norm_s, norm_r, save_sem,
):
    f32, bf16 = jnp.float32, jnp.bfloat16
    fs_at = lax.axis_index("fs")
    tp_at = lax.axis_index("tp")
    a_at, b_at = fs_at // fb, fs_at % fb
    z_at, c_at = tp_at // CORES, tp_at % CORES
    hidden, rows = up_gate_ref.shape
    shard, width = tok_ref.shape
    block = gw_ref.shape[1]
    wide = fa * block
    piece = CORES * shard
    chunks = hidden_chunks(hidden)
    shifts = piece_shifts(chips)
    steps, ready = stream_steps(len(chunks), chips)
    tp_size = chips * CORES
    fs_size = fa * fb

    def x_peer(d):
        return (a_at * fb + (b_at + d) % fb, tp_at)

    def y_peer(d):
        return (((a_at + d) % fa) * fb + b_at, tp_at)

    def z_peer(z):
        return (fs_at, z * CORES + c_at)

    core_peer = (fs_at, z_at * CORES + (CORES - 1 - c_at))

    def remote(src, dst, send, recv, peer):
        return pltpu.make_async_remote_copy(
            src_ref=src, dst_ref=dst, send_sem=send, recv_sem=recv, device_id=peer, device_id_type=MESH
        )

    barrier = pltpu.get_barrier_semaphore()
    peers = [((fs_at + d) % fs_size, tp_at) for d in range(1, fs_size)]
    peers += [(fs_at, (tp_at + d) % tp_size) for d in range(1, tp_size)]
    for peer in peers:
        pl.semaphore_signal(barrier, inc=1, device_id=peer, device_id_type=MESH)

    loads = []

    def distance(u, v):
        return jnp.abs(u - v)

    def may_be_two(shift):
        return shift == 2 or chips - shift == 2

    def must_be_two(shift):
        return shift == 2 and chips - shift == 2

    def load(src, dst):
        copy = pltpu.make_async_copy(src, dst, load_sem.at[len(loads)])
        copy.start()
        loads.append(copy)
        return copy

    tap_loads = [load(gate_taps_ref, gtaps), load(val_taps_ref, vtaps)]
    first_loads = [load(tok_ref, held), load(gw_ref, wg.at[0]), load(vw_ref, wv.at[0])]
    field_loads = []
    first = chunks[0][1]
    for cut in [pl.ds(0, first)] + ([pl.ds(first, hidden - first)] if hidden > first else []):
        field_loads.append(
            [load(s.at[cut], d.at[cut]) for s, d in ((up_gate_ref, fg), (up_val_ref, fv), (grad_ref, fh))]
        )

    def token_columns(ref, d, d_a):
        start = (((a_at + d_a) % fa) * fb + (b_at + d) % fb) * block
        return ref.at[:, pl.ds(pl.multiple_of(start, block), block)]

    def token_rows(z, c):
        return pl.ds(pl.multiple_of((z * CORES + c) * shard, shard), shard)

    mine = token_rows(z_at, c_at)
    tok_loads = [
        load(token_columns(tok_ref, 0, d_a), tok.at[0, mine, pl.ds(d_a * block, block)]) for d_a in range(fa)
    ]

    middle = jnp.logical_and(z_at >= 1, z_at <= chips - 2)

    @pl.when(jnp.logical_not(middle))
    def _():
        relayed[...] = jnp.zeros_like(relayed)

    for j, shift in enumerate(shifts):
        if may_be_two(shift) and not must_be_two(shift):
            @pl.when(distance((z_at + chips - shift) % chips, z_at) == 2)
            def _(j=j):
                zrecv[:, j] = jnp.zeros_like(zrecv[:, j])

    for copy in tap_loads:
        copy.wait()
    kern_in[...] = jnp.zeros_like(kern_in)
    kern_in[0:taps, 0:hidden] = gtaps[...].astype(f32)
    kern_in[taps : 2 * taps, 0:hidden] = vtaps[...].astype(f32)
    kern_ref[...] = kern_in[...].T

    for copy in first_loads:
        copy.wait()
    pl.semaphore_wait(barrier, len(peers))

    sends = []

    def send(copy):
        copy.start()
        sends.append(copy)
        return copy

    tokx = {}
    for d in range(1, fb):
        for d_a in range(fa):
            send(remote(
                token_columns(held, d, d_a), tok.at[fb - d, mine, pl.ds(d_a * block, block)],
                tokx_s.at[d - 1, d_a], tokx_r.at[fb - d - 1, d_a], x_peer(d),
            ))
            tokx[fb - d, d_a] = sends[-1]
    w_waits = {}
    for d in range(1, fa):
        for i, dst in enumerate((wg, wv)):
            src = dst.at[0]
            send(remote(src, dst.at[fa - d], w_s.at[d - 1, i], w_r.at[fa - d - 1, i], y_peer(d)))
            w_waits[fa - d, i] = remote(
                src, dst.at[fa - d], w_s.at[d - 1, i], w_r.at[fa - d - 1, i], y_peer(d)
            )

    late = []

    def tok_z(s):
        for j in range(1, chips):
            to = (z_at + j) % chips

            copy = remote(
                tok.at[s, mine], tok.at[s, mine], tokz_s.at[s, j - 1], tokz_r.at[s, z_at], z_peer(to)
            )
            direct = distance(to, z_at) != 2

            @pl.when(direct)
            def _(copy=copy):
                copy.start()

            late.append((direct, copy))
        send(remote(tok.at[s, mine], tok.at[s, mine], tokc_s.at[s, z_at], tokc_r.at[s, z_at], core_peer))

    def tok_arrived(s, source):
        at = token_rows(source, c_at)
        remote(tok.at[s, at], tok.at[s, at], tokz_s.at[s, 0], tokz_r.at[s, source], z_peer(z_at)).wait_recv()

    def to_core(s, source):
        at = token_rows(source, c_at)
        send(remote(tok.at[s, at], tok.at[s, at], tokc_s.at[s, source], tokc_r.at[s, source], core_peer))

    def tok_relay(s):
        for side, step in enumerate((1, -1)):
            source, target = z_at - step, z_at + step
            exists = jnp.logical_and(source >= 0, source < chips)
            both = jnp.logical_and(exists, jnp.logical_and(target >= 0, target < chips))
            source = (source + chips) % chips
            target = (target + chips) % chips
            at = token_rows(source, c_at)
            copy = remote(
                tok.at[s, at], tok.at[s, at], relay_s.at[s, side], tokz_r.at[s, source], z_peer(target)
            )

            @pl.when(exists)
            def _(source=source):
                tok_arrived(s, source)

            @pl.when(both)
            def _(copy=copy):
                copy.start()

            late.append((both, copy))

            forward = remote(
                tok.at[s, at], tok.at[s, at], tokc_s.at[s, source], tokc_r.at[s, source], core_peer
            )

            @pl.when(exists)
            def _(forward=forward):
                forward.start()

            late.append((exists, forward))

    def tok_rest(s):
        for j in range(1, chips):
            source = (z_at + j) % chips
            far = distance(source, z_at) > 1
            at = token_rows(source, c_at)
            forward = remote(
                tok.at[s, at], tok.at[s, at], tokc_s.at[s, source], tokc_r.at[s, source], core_peer
            )

            @pl.when(far)
            def _(source=source, forward=forward):
                tok_arrived(s, source)
                forward.start()

            late.append((far, forward))

    def tok_from_core(s):
        for z in range(chips):
            at = token_rows(z, CORES - 1 - c_at)
            remote(tok.at[s, at], tok.at[s, at], tokc_s.at[s, z], tokc_r.at[s, z], core_peer).wait_recv()

    def lanes(j):
        return pl.ds(pl.multiple_of(((z_at + shifts[j]) % chips) * piece, piece), piece)

    def back_slice(slot, step):
        lo, hi, j = steps[step]
        first = 2 * chunks[lo][0]
        last = 2 * (chunks[hi - 1][0] + chunks[hi - 1][1])
        if j is None:
            return back.at[slot, pl.ds(first, last - first)]
        return back.at[slot, pl.ds(first, last - first), lanes(j)]


    def send_back(step):
        for d in range(1, fb):
            copy = remote(
                back_slice(0, step), back_slice(fb - d, step),
                back_s.at[d - 1], back_r.at[fb - d - 1, step], x_peer(d),
            )
            copy.start()

    got = [0]

    def await_back(until):
        while got[0] < until:
            step = got[0]
            for s in range(1, fb):
                remote(
                    back_slice(0, step), back_slice(s, step),
                    back_s.at[0], back_r.at[s - 1, step], x_peer(1 % fb),
                ).wait_recv()
            got[0] += 1

    if tapbuf.shape[0] > hidden:
        tapbuf[hidden:, :] = jnp.zeros((tapbuf.shape[0] - hidden, 128), f32)

    for copy in tok_loads:
        copy.wait()
    tok_z(0)
    next_step = 0
    after_conv = {min(1, len(chunks) - 1): [lambda: [tok_x_done(), [tok_z(s) for s in range(1, fb)]]]}

    def tok_x_done():
        for s in range(1, fb):
            for d_a in range(fa):
                tokx[s, d_a].wait_recv()

    relays = list(range(fb))
    for k, (at, size) in enumerate(chunks):
        if k < len(field_loads):
            for copy in field_loads[k]:
                copy.wait()
        group = 16 if size % 16 == 0 else 8
        conv_rows(group, rows, taps, at, 2 * at, size, fg, fv, fh, kern_ref, back, tapbuf)
        while next_step < len(steps) and steps[next_step][1] <= k + 1:
            send_back(next_step)
            next_step += 1
        for action in after_conv.get(k, []):
            action()
        if k == 3:
            tok_relay(relays.pop(0))

    tap_t = tapbuf[...].T
    tapx[fs_at] = tap_t[0 : tapx.shape[1], :]
    for d in range(1, fs_size):
        to = ((fs_at + d) % fs_size, tp_at)
        copy = remote(tapx.at[fs_at], tapx.at[fs_at], tap_s.at[0], tap_r.at[fs_at], to)
        copy.start()

    def transpose_weights(d):
        for at, size in chunks:
            pair = jnp.concatenate((wg[d, pl.ds(at, size), :], wv[d, pl.ds(at, size), :]), axis=0)
            wt[pl.ds(d * block, block), pl.ds(2 * at, 2 * size)] = pair.T

    inner = (((1,), (0,)), ((), ()))
    mblock = min(256, block)

    def rows_of(ref, r, j, d):
        return ref.at[r, j, pl.ds(d * block, block)]

    def core_copy(r, j, d):
        return remote(
            rows_of(psend, r, j, d), rows_of(precv, r, j, d), pc_s.at[0], pc_r.at[r, j, d], core_peer
        )

    def partial(r, j, d):
        right = back[r, :, lanes(j)]

        def one(i, carry):
            at = pl.ds(pl.multiple_of(d * block + i * mblock, mblock), mblock)
            out = lax.dot_general(wt[at, :], right, inner, preferred_element_type=f32).astype(bf16)
            own = jnp.where(c_at == 0, out[:, 0:shard], out[:, shard:piece])
            other = jnp.where(c_at == 0, out[:, shard:piece], out[:, 0:shard])
            pown[r, j, at, :] = own
            psend[r, j, at, :] = other
            return carry

        lax.fori_loop(0, block // mblock, one, 0)
        core_copy(r, j, d).start()

    def relay_copy(r, j, d, side, peer):
        return remote(
            rows_of(ssend, r, j, d), relayed.at[r, side, pl.ds(d * block, block)],
            pz_s.at[r, j, d], mid_r.at[r, side, d], peer,
        )

    def chip_copy(r, j, d, peer):
        return remote(
            rows_of(ssend, r, j, d), rows_of(zrecv, r, j, d), pz_s.at[r, j, d], pz_r.at[r, j, d], peer
        )

    def reduce_core(r, j, d):
        core_copy(r, j, d).wait_recv()
        cut = slice(d * block, (d + 1) * block)
        total = pown[r, j, cut].astype(f32) + precv[r, j, cut].astype(f32)
        shift = shifts[j]
        if chips > 2 and shift in (1, chips - 1):
            side = 0 if shift == 1 else 1

            @pl.when(middle)
            def _():
                relay_copy(r, j, d, side, z_peer(z_at)).wait_recv()

            total = total + relayed[r, side, cut].astype(f32)
        ssend[r, j, cut] = total.astype(bf16)
        if shift == 0:
            return
        to = (z_at + shift) % chips
        if not must_be_two(shift):
            direct = distance(to, z_at) != 2
            copy = chip_copy(r, j, d, z_peer(to))
            late.append((direct, copy))

            @pl.when(direct)
            def _():
                copy.start()
        if may_be_two(shift):
            for side, step in enumerate((1, -1)):
                through = to == z_at + 2 * step
                relay = relay_copy(r, j, d, side, z_peer((z_at + step + chips) % chips))
                late.append((through, relay))

                @pl.when(through)
                def _(relay=relay):
                    relay.start()

    def reduce_chips(r, d):
        cut = slice(d * block, (d + 1) * block)
        total = ssend[r, chips - 1, cut].astype(f32)
        for j in range(chips - 1):
            if must_be_two(shifts[j]):
                continue

            @pl.when(distance((z_at + chips - shifts[j]) % chips, z_at) != 2)
            def _(j=j):
                chip_copy(r, j, d, z_peer(z_at)).wait_recv()

            total = total + zrecv[r, j, cut].astype(f32)
        return total.astype(bf16).T

    saves = []

    def save(src, dst):
        copy = pltpu.make_async_copy(src, dst, save_sem.at[len(saves)])
        copy.start()
        saves.append(copy)

    def gradient(k):
        at, size = chunks[k]
        cut = pl.ds(2 * at, 2 * size)
        for d_a in list(range(1, fa)) + [0]:
            cols = slice(d_a * block, (d_a + 1) * block)
            total = lax.dot_general(back[0, cut, :], tok[0, :, cols], inner, preferred_element_type=f32)
            for s in range(1, fb):
                total = total + lax.dot_general(
                    back[s, cut, :], tok[s, :, cols], inner, preferred_element_type=f32
                )
            if d_a:
                gsend[d_a - 1, cut, :] = total.astype(bf16)
                remote(
                    gsend.at[d_a - 1, cut], grecv.at[fa - d_a - 1, cut],
                    g_s.at[d_a - 1], g_r.at[fa - d_a - 1, k], y_peer(d_a),
                ).start()
            else:
                gate_out[pl.ds(at, size), :] = total[:size]
                val_out[pl.ds(at, size), :] = total[size:]

    def finish_gradient(k, norms):
        at, size = chunks[k]
        cut = pl.ds(2 * at, 2 * size)
        for s in range(1, fa):
            remote(
                gsend.at[s - 1, cut], grecv.at[s - 1, cut], g_s.at[s - 1], g_r.at[s - 1, k], y_peer(1 % fa)
            ).wait_recv()
        new = []
        for i, out in enumerate((gate_out, val_out)):
            rows_at = pl.ds(at, size)
            total = out[rows_at, :]
            for s in range(1, fa):
                total = total + grecv[s - 1, pl.ds(2 * at + i * size, size), :].astype(f32)
            out[rows_at, :] = total
            new.append(norms[i] + jnp.sum(total * total, axis=0, keepdims=True))
        if k in (len(chunks) - 4, len(chunks) - 1):
            low = 0 if k == len(chunks) - 4 or len(chunks) < 4 else chunks[len(chunks) - 3][0]
            whole = pl.ds(low, at + size - low)
            save(gate_out.at[whole], gate_done.at[whole])
            save(val_out.at[whole], val_done.at[whole])
        return new

    transpose_weights(0)
    for j in range(chips):
        partial(0, j, 0)
        if j == min(1, chips - 1):
            while relays:
                tok_relay(relays.pop(0))
    for d in range(1, fa):
        for i in range(2):
            w_waits[d, i].wait_recv()
        transpose_weights(d)
        for j in range(chips):
            partial(0, j, d)
            if d == 1 and j == 0:
                reduce_core(0, 0, 0)
            if j == min(1, chips - 1):
                reduce_core(0, 0, d)
    for s in range(fb):
        tok_rest(s)
    for j in range(1, chips):
        for d in range(fa):
            reduce_core(0, j, d)
    for s in range(fb):
        tok_from_core(s)

    def place(slot, d_a, value):
        start = (((a_at + d_a) % fa) * fb + (b_at + slot) % fb) * block
        cut = pl.ds(pl.multiple_of(start, block), block)
        dx_ref[slot, :, d_a * block : (d_a + 1) * block] = value
        save(dx_ref.at[slot, :, pl.ds(d_a * block, block)], dx_out.at[:, cut])

    norms = [jnp.zeros((1, block), f32), jnp.zeros((1, block), f32)]
    waiting, finished = [], 0

    for kind, index, until in ready:
        await_back(until)
        if kind == "chunk":
            gradient(index)
            for item in waiting:
                reduce_core(*item)
            waiting = []
            if finished <= index - 3 and until < len(steps) - 2:
                norms = finish_gradient(finished, norms)
                finished += 1
        else:
            for item in waiting:
                reduce_core(*item)
            waiting = []
            for r in range(1, fb):
                for d in range(fa):
                    partial(r, index, d)
                    waiting.append((r, index, d))
            if index == chips - 2:
                for item in waiting:
                    reduce_core(*item)
                waiting = []
    for d in range(fa):
        place(0, d, reduce_chips(0, d))
    for r in range(1, fb):
        for d in range(fa):
            for item in waiting:
                if item[0] == r and item[2] == d:
                    reduce_core(*item)
            cut = pl.ds(d * block, block)
            xsend[r - 1, :, cut] = reduce_chips(r, d)
            send(remote(
                xsend.at[r - 1, :, cut], xrecv.at[fb - r - 1, :, cut],
                out_s.at[r - 1, d], out_r.at[fb - r - 1, d], x_peer(r),
            ))

    tap_total = None
    for f in range(fs_size):
        @pl.when(fs_at != f)
        def _(f=f):
            remote(tapx.at[f], tapx.at[f], tap_s.at[0], tap_r.at[f], (fs_at, tp_at)).wait_recv()

        tap_total = tapx[f] if f == 0 else tap_total + tapx[f]
    tap_held[...] = tap_total
    save(tap_held, tap_out)
    tap_norms = jnp.sum(tap_total * tap_total, axis=1, keepdims=True)
    normx[tp_at, 2 : 2 + 2 * taps, :] = jnp.broadcast_to(tap_norms[0 : 2 * taps], (2 * taps, block))

    for k in range(finished, len(chunks)):
        norms = finish_gradient(k, norms)
    normx[tp_at, 0:1, :] = norms[0]
    normx[tp_at, 1:2, :] = norms[1]
    for d in range(1, tp_size):
        to = (fs_at, (tp_at + d) % tp_size)
        remote(normx.at[tp_at], normx.at[tp_at], norm_s.at[0], norm_r.at[tp_at], to).start()

    for s in range(1, fb):
        for d in range(fa):
            cut = pl.ds(d * block, block)
            remote(
                xsend.at[s - 1, :, cut], xrecv.at[s - 1, :, cut],
                out_s.at[s - 1, d], out_r.at[s - 1, d], x_peer(1 % fb),
            ).wait_recv()
            start = (((a_at + d) % fa) * fb + (b_at + s) % fb) * block
            save(xrecv.at[s - 1, :, cut], dx_out.at[:, pl.ds(pl.multiple_of(start, block), block)])

    norm_total = None
    for t in range(tp_size):
        @pl.when(tp_at != t)
        def _(t=t):
            remote(normx.at[t], normx.at[t], norm_s.at[0], norm_r.at[t], (fs_at, tp_at)).wait_recv()

        norm_total = normx[t] if t == 0 else norm_total + normx[t]
    norm_held[...] = norm_total
    save(norm_held, norm_out)

    for copy in saves:
        copy.wait()
    for d in range(1, fb):
        remote(back.at[0], back.at[fb - d], back_s.at[d - 1], back_r.at[fb - d - 1, 0], x_peer(d)).wait_send()
    for d in range(1, fa):
        remote(
            gsend.at[d - 1], grecv.at[fa - d - 1], g_s.at[d - 1], g_r.at[fa - d - 1, 0], y_peer(d)
        ).wait_send()
    remote(psend, precv, pc_s.at[0], pc_r.at[0, 0, 0], core_peer).wait_send()
    if fs_size > 1:
        others = tapx.at[pl.ds(0, fs_size - 1)]
        remote(others, others, tap_s.at[0], tap_r.at[0], x_peer(1 % fb)).wait_send()
    others = normx.at[pl.ds(0, tp_size - 1)]
    remote(others, others, norm_s.at[0], norm_r.at[0], core_peer).wait_send()
    for copy in sends:
        copy.wait_send()
    for started, copy in late:
        @pl.when(started)
        def _(copy=copy):
            copy.wait_send()


def whole_step(fa, fb, chips, taps, tokens, up_gate, up_val, gate_weight, val_weight, gate_taps, val_taps, hidden_grad):
    f32, bf16 = jnp.float32, jnp.bfloat16
    hidden, rows = up_gate.shape
    shard, width = tokens.shape
    block = gate_weight.shape[1]
    wide = fa * block
    fs_size, tp_size = fa * fb, chips * CORES
    chunks = hidden_chunks(hidden)
    n = len(chunks)
    steps, _ = stream_steps(n, chips)
    padded = -(-hidden // 128) * 128
    tap_rows = -(-2 * taps // 8) * 8
    norm_rows = -(-(2 + 2 * taps) // 8) * 8
    dma = pltpu.SemaphoreType.DMA
    xs, ys = max(1, fb - 1), max(1, fa - 1)
    scratch = [
        pltpu.VMEM((hidden, rows), bf16),
        pltpu.VMEM((hidden, rows), bf16),
        pltpu.VMEM((hidden, rows), bf16),
        pltpu.VMEM((fb, rows, wide), bf16),
        pltpu.VMEM((fb, 2 * hidden, rows), bf16),
        pltpu.VMEM((fa, hidden, block), bf16),
        pltpu.VMEM((fa, hidden, block), bf16),
        pltpu.VMEM((wide, 2 * hidden), bf16),
        pltpu.VMEM((fb, chips, wide, shard), bf16),
        pltpu.VMEM((fb, chips, wide, shard), bf16),
        pltpu.VMEM((fb, chips, wide, shard), bf16),
        pltpu.VMEM((fb, chips, wide, shard), bf16),
        pltpu.VMEM((fb, chips, wide, shard), bf16),
        pltpu.VMEM((xs, shard, wide), bf16),
        pltpu.VMEM((xs, shard, wide), bf16),
        pltpu.VMEM((ys, 2 * hidden, block), bf16),
        pltpu.VMEM((ys, 2 * hidden, block), bf16),
        pltpu.VMEM((padded, 128), f32),
        pltpu.VMEM((fs_size, tap_rows, padded), f32),
        pltpu.VMEM((tp_size, norm_rows, block), f32),
        pltpu.VMEM((fb, 2, wide, shard), bf16),
        pltpu.VMEM((taps, hidden), bf16),
        pltpu.VMEM((taps, hidden), bf16),
        pltpu.VMEM((128, padded), f32),
        pltpu.VMEM((padded, 128), f32),
        pltpu.VMEM((1, shard, wide), bf16),
        pltpu.VMEM((hidden, block), f32),
        pltpu.VMEM((hidden, block), f32),
        pltpu.VMEM((shard, width), bf16),
        pltpu.VMEM((tap_rows, padded), f32),
        pltpu.VMEM((norm_rows, block), f32),
        dma((fa + 11,)),
        dma((xs, fa)),
        dma((xs, fa)),
        dma((fb, max(1, chips - 1))),
        dma((fb, chips)),
        dma((fb, 2)),
        dma((fb, chips)),
        dma((fb, chips)),
        dma((ys, 2)),
        dma((ys, 2)),
        dma((xs,)),
        dma((xs, len(steps))),
        dma((1,)),
        dma((fb, chips, fa)),
        dma((fb, max(1, chips - 1), fa)),
        dma((fb, max(1, chips - 1), fa)),
        dma((fb, 2, fa)),
        dma((xs, fa)),
        dma((xs, fa)),
        dma((ys,)),
        dma((ys, n)),
        dma((1,)),
        dma((fs_size,)),
        dma((1,)),
        dma((tp_size,)),
        dma((fs_size + 6,)),
    ]
    return pl.pallas_call(
        functools.partial(step_kernel, fa, fb, chips, taps),
        in_specs=[HBM] * 8,
        out_specs=[ANY] * 5,
        out_shape=[
            jax.ShapeDtypeStruct((shard, width), bf16),
            jax.ShapeDtypeStruct((hidden, block), f32),
            jax.ShapeDtypeStruct((hidden, block), f32),
            jax.ShapeDtypeStruct((tap_rows, padded), f32),
            jax.ShapeDtypeStruct((norm_rows, block), f32),
        ],
        scratch_shapes=scratch,
        compiler_params=pltpu.CompilerParams(
            collective_id=0, has_side_effects=True, vmem_limit_bytes=VMEM_LIMIT
        ),
    )(tokens, up_gate, up_val, gate_weight, val_weight, gate_taps, val_taps, hidden_grad)


def results_kernel(
    taps, hidden, dx_in, gate_in, val_in, tap_in, norm_in,
    dx_out, gate_out, val_out, gate_tap, val_tap, gate_norm, val_norm, tap_norm,
    dx, gate, val, tap, norm, gate_tap_held, val_tap_held, gate_norm_held, val_norm_held, tap_norm_held,
    in_sem, out_sem,
):
    half = hidden // 16 * 8
    parts = [(tap_in, tap, None), (norm_in, norm, None)]
    for cut in (pl.ds(0, half), pl.ds(half, hidden - half)):
        for src, held, dst in ((gate_in, gate, gate_out), (val_in, val, val_out)):
            parts.append((src.at[cut], held.at[cut], dst.at[cut]))
    parts.append((dx_in, dx, dx_out))
    ins = [pltpu.make_async_copy(src, held, in_sem.at[i]) for i, (src, held, _) in enumerate(parts)]
    for copy in ins:
        copy.start()
    outs = []

    def out(held, dst):
        outs.append(pltpu.make_async_copy(held, dst, out_sem.at[len(outs)]))
        outs[-1].start()

    ins[0].wait()
    gate_tap_held[...] = tap[0:taps, 0:hidden]
    val_tap_held[...] = tap[taps : 2 * taps, 0:hidden]
    ins[1].wait()
    gate_norm_held[...] = norm[0, :]
    val_norm_held[...] = norm[1, :]
    for i in range(2):
        for t in range(taps):
            tap_norm_held[i : i + 1, t : t + 1] = norm[2 + i * taps + t : 3 + i * taps + t, 0:1]
    for held, dst in (
        (gate_tap_held, gate_tap), (val_tap_held, val_tap), (gate_norm_held, gate_norm),
        (val_norm_held, val_norm), (tap_norm_held, tap_norm),
    ):
        out(held, dst)
    for i, (_, held, dst) in enumerate(parts):
        if dst is not None:
            ins[i].wait()
        if dst is not None:
            out(held, dst)
    for copy in outs:
        copy.wait()


def results(taps, hidden, dx, gate, val, tap, norm):
    f32 = jnp.float32
    block = norm.shape[1]
    small = [((taps, hidden), f32)] * 2 + [((block,), f32)] * 2 + [((2, taps), f32)]
    return pl.pallas_call(
        functools.partial(results_kernel, taps, hidden),
        in_specs=[ANY] * 5,
        out_specs=[ANY] * 8,
        out_shape=[jax.ShapeDtypeStruct(v.shape, v.dtype) for v in (dx, gate, val)]
        + [jax.ShapeDtypeStruct(*kind) for kind in small],
        scratch_shapes=[pltpu.VMEM(v.shape, v.dtype) for v in (dx, gate, val, tap, norm)]
        + [pltpu.VMEM(*kind) for kind in small]
        + [pltpu.SemaphoreType.DMA((7,)), pltpu.SemaphoreType.DMA((10,))],
        compiler_params=pltpu.CompilerParams(vmem_limit_bytes=VMEM_LIMIT),
    )(dx, gate, val, tap, norm)


def solution(mesh):
    fs_size, tp_size = mesh.shape["fs"], mesh.shape["tp"]
    fb = max(d for d in range(1, fs_size + 1) if fs_size % d == 0 and d * d <= fs_size)
    fa = fs_size // fb
    chips = tp_size // CORES

    def local(tokens, up_gate, up_val, gate_weight, val_weight, gate_taps, val_taps, hidden_grad):
        taps, hidden = gate_taps.shape
        dx, gate_grad, val_grad, tap_grad, norms = whole_step(
            fa, fb, chips, taps, tokens, up_gate.T, up_val.T, gate_weight.T, val_weight.T,
            gate_taps, val_taps, hidden_grad.T,
        )
        dx, gate_grad, val_grad, gate_tap, val_tap, gate_norm, val_norm, tap_norm = results(
            taps, hidden, dx, gate_grad, val_grad, tap_grad, norms
        )
        return dx, gate_grad.T, val_grad.T, gate_tap, val_tap, gate_norm, val_norm, tap_norm

    in_specs = (
        P(("fs", "tp"), None),
        P("fs", "tp"),
        P("fs", "tp"),
        P("fs", "tp"),
        P("fs", "tp"),
        P(None, "tp"),
        P(None, "tp"),
        P("fs", "tp"),
    )
    out_specs = (
        P(("fs", "tp"), None),
        P("fs", "tp"),
        P("fs", "tp"),
        P(None, "tp"),
        P(None, "tp"),
        P("fs"),
        P("fs"),
        P(),
    )
    return jax.shard_map(local, mesh=mesh, in_specs=in_specs, out_specs=out_specs, check_vma=False)
```

```python
import functools

import jax
import jax.numpy as jnp
from jax import lax
from jax.experimental import pallas as pl
from jax.experimental.pallas import tpu as pltpu
from jax.sharding import PartitionSpec as P

SEQ = 1024
CORES = 2
VMEM_LIMIT = 60 * 1024 * 1024
MESH = pl.DeviceIdType.MESH
ANY = pl.BlockSpec(memory_space=pl.ANY)
HBM = pl.BlockSpec(memory_space=pltpu.HBM)
VMEM = pl.BlockSpec(memory_space=pltpu.VMEM)


def hidden_chunks(hidden):
    if hidden % 64:
        return [(0, hidden)]
    units = hidden // 64
    small = min(5, units)
    small += (units - small) % 2
    sizes = [128] * ((units - small) // 2) + [64] * small
    chunks, at = [], 0
    for size in sizes:
        chunks.append((at, size))
        at += size
    return chunks


def piece_shifts(chips):
    return sorted(range(1, chips), key=lambda s: (-min(s, chips - s), s)) + [0]


def stream_steps(n, pieces):
    steps, ready = [], []
    heads = n - min(2, n)
    lead = max(0, min(2, heads - 1))

    def rest(k, j):
        for later in range(j + 1, pieces):
            steps.append((k, k + 1, later))
        ready.append(("chunk", k, len(steps)))

    for k in range(lead):
        steps.append((k, k + 1, None))
        ready.append(("chunk", k, len(steps)))
    for j in range(pieces - 1):
        steps.append((lead, n, j))
        ready.append(("piece", j, len(steps)))
        last = lead + 1 if j < pieces - 3 else heads
        while j < pieces - 2 and lead < min(last, heads):
            rest(lead, j)
            lead += 1
    for k in range(lead, n):
        steps.append((k, k + 1, pieces - 1))
        ready.append(("chunk", k, len(steps)))
    ready.append(("piece", pieces - 1, len(steps)))
    return steps, ready


def conv_rows(group, rows, taps, at, base, size, gate_ref, val_ref, grad_ref, kern_ref, back_ref, tap_ref):
    place = lax.broadcasted_iota(jnp.int32, (group, rows), 1) % SEQ
    lane = lax.broadcasted_iota(jnp.int32, (group, 128), 1)

    def one(index, carry):
        here = pl.multiple_of(at + index * group, group)
        src = pl.ds(here, group)
        kernels = kern_ref[src, :]
        gate_kernel = kernels[:, 0:taps]
        val_kernel = kernels[:, taps : 2 * taps]

        def delayed(field, shift):
            if shift == 0:
                return field
            return jnp.where(place >= shift, pltpu.roll(field, shift, 1), 0.0)

        def advanced(field, shift):
            if shift == 0:
                return field
            return jnp.where(place < SEQ - shift, pltpu.roll(field, rows - shift, 1), 0.0)

        def mixed(fields, kernel):
            total = fields[0] * kernel[:, 0:1]
            for i in range(1, taps):
                total = total + fields[i] * kernel[:, i : i + 1]
            return total

        gate = gate_ref[src, :].astype(jnp.float32)
        val = val_ref[src, :].astype(jnp.float32)
        gate_fields = [delayed(gate, taps - 1 - i) for i in range(taps)]
        val_fields = [delayed(val, taps - 1 - i) for i in range(taps)]
        conv_gate = mixed(gate_fields, gate_kernel)
        conv_val = mixed(val_fields, val_kernel)
        sigmoid = jax.nn.sigmoid(conv_gate)
        scaled = grad_ref[src, :].astype(jnp.float32) * sigmoid
        val_back = scaled * conv_gate
        gate_back = scaled * conv_val * (1.0 + conv_gate * (1.0 - sigmoid))
        row = pl.multiple_of(base + index * group, group)
        back_ref[0, pl.ds(row, group), :] = mixed(
            [advanced(gate_back, taps - 1 - i) for i in range(taps)], gate_kernel
        ).astype(jnp.bfloat16)
        row = pl.multiple_of(base + size + index * group, group)
        back_ref[0, pl.ds(row, group), :] = mixed(
            [advanced(val_back, taps - 1 - i) for i in range(taps)], val_kernel
        ).astype(jnp.bfloat16)
        sums = jnp.zeros((group, 128), jnp.float32)
        for i in range(taps):
            sums = jnp.where(lane == i, jnp.sum(gate_fields[i] * gate_back, axis=1, keepdims=True), sums)
            sums = jnp.where(
                lane == taps + i, jnp.sum(val_fields[i] * val_back, axis=1, keepdims=True), sums
            )
        tap_ref[src, :] = sums
        return carry

    lax.fori_loop(0, size // group, one, 0)


def step_kernel(
    fa, fb, chips, taps,
    tok_ref, up_gate_ref, up_val_ref, gw_ref, vw_ref, gate_taps_ref, val_taps_ref, grad_ref,
    dx_out, gate_done, val_done, tap_out, norm_out,
    fg, fv, fh, tok, back, wg, wv, wt, pown, psend, precv, ssend, zrecv, xsend, xrecv,
    gsend, grecv, tapbuf, tapx, normx, relayed, gtaps, vtaps, kern_in, kern_ref, dx_ref, gate_out, val_out, held, tap_held, norm_held, acc,
    load_sem, tokx_s, tokx_r, tokz_s, tokz_r, relay_s, tokc_s, tokc_r, w_s, w_r,
    back_s, back_r, pc_s, pc_r, pz_s, pz_r, mid_r, out_s, out_r, g_s, g_r, tap_s, tap_r, norm_s, norm_r, save_sem,
):
    f32, bf16 = jnp.float32, jnp.bfloat16
    fs_at = lax.axis_index("fs")
    tp_at = lax.axis_index("tp")
    a_at, b_at = fs_at // fb, fs_at % fb
    z_at, c_at = tp_at // CORES, tp_at % CORES
    hidden, rows = up_gate_ref.shape
    shard, width = tok_ref.shape
    block = gw_ref.shape[1]
    wide = fa * block
    piece = CORES * shard
    chunks = hidden_chunks(hidden)
    shifts = piece_shifts(chips)
    steps, ready = stream_steps(len(chunks), chips)
    tp_size = chips * CORES
    fs_size = fa * fb

    def x_peer(d):
        return (a_at * fb + (b_at + d) % fb, tp_at)

    def y_peer(d):
        return (((a_at + d) % fa) * fb + b_at, tp_at)

    def z_peer(z):
        return (fs_at, z * CORES + c_at)

    core_peer = (fs_at, z_at * CORES + (CORES - 1 - c_at))

    def remote(src, dst, send, recv, peer):
        return pltpu.make_async_remote_copy(
            src_ref=src, dst_ref=dst, send_sem=send, recv_sem=recv, device_id=peer, device_id_type=MESH
        )

    barrier = pltpu.get_barrier_semaphore()
    peers = [((fs_at + d) % fs_size, tp_at) for d in range(1, fs_size)]
    peers += [(fs_at, (tp_at + d) % tp_size) for d in range(1, tp_size)]
    for peer in peers:
        pl.semaphore_signal(barrier, inc=1, device_id=peer, device_id_type=MESH)

    loads = []

    def distance(u, v):
        return jnp.abs(u - v)

    def may_be_two(shift):
        return shift == 2 or chips - shift == 2

    def must_be_two(shift):
        return shift == 2 and chips - shift == 2

    def load(src, dst):
        copy = pltpu.make_async_copy(src, dst, load_sem.at[len(loads)])
        copy.start()
        loads.append(copy)
        return copy

    tap_loads = [load(gate_taps_ref, gtaps), load(val_taps_ref, vtaps)]
    first_loads = [load(tok_ref, held), load(gw_ref, wg.at[0]), load(vw_ref, wv.at[0])]
    field_loads = []
    first = chunks[0][1]
    for cut in [pl.ds(0, first)] + ([pl.ds(first, hidden - first)] if hidden > first else []):
        field_loads.append(
            [load(s.at[cut], d.at[cut]) for s, d in ((up_gate_ref, fg), (up_val_ref, fv), (grad_ref, fh))]
        )

    def token_columns(ref, d, d_a):
        start = (((a_at + d_a) % fa) * fb + (b_at + d) % fb) * block
        return ref.at[:, pl.ds(pl.multiple_of(start, block), block)]

    def token_rows(z, c):
        return pl.ds(pl.multiple_of((z * CORES + c) * shard, shard), shard)

    mine = token_rows(z_at, c_at)
    tok_loads = [
        load(token_columns(tok_ref, 0, d_a), tok.at[0, mine, pl.ds(d_a * block, block)]) for d_a in range(fa)
    ]

    middle = jnp.logical_and(z_at >= 1, z_at <= chips - 2)

    @pl.when(jnp.logical_not(middle))
    def _():
        relayed[...] = jnp.zeros_like(relayed)

    for j, shift in enumerate(shifts):
        if may_be_two(shift) and not must_be_two(shift):
            @pl.when(distance((z_at + chips - shift) % chips, z_at) == 2)
            def _(j=j):
                zrecv[:, j] = jnp.zeros_like(zrecv[:, j])

    for copy in tap_loads:
        copy.wait()
    kern_in[...] = jnp.zeros_like(kern_in)
    kern_in[0:taps, 0:hidden] = gtaps[...].astype(f32)
    kern_in[taps : 2 * taps, 0:hidden] = vtaps[...].astype(f32)
    kern_ref[...] = kern_in[...].T

    for copy in first_loads:
        copy.wait()
    pl.semaphore_wait(barrier, len(peers))

    sends = []

    def send(copy):
        copy.start()
        sends.append(copy)
        return copy

    tokx = {}
    for d in range(1, fb):
        for d_a in range(fa):
            send(remote(
                token_columns(held, d, d_a), tok.at[fb - d, mine, pl.ds(d_a * block, block)],
                tokx_s.at[d - 1, d_a], tokx_r.at[fb - d - 1, d_a], x_peer(d),
            ))
            tokx[fb - d, d_a] = sends[-1]
    w_waits = {}
    for d in range(1, fa):
        for i, dst in enumerate((wg, wv)):
            src = dst.at[0]
            send(remote(src, dst.at[fa - d], w_s.at[d - 1, i], w_r.at[fa - d - 1, i], y_peer(d)))
            w_waits[fa - d, i] = remote(
                src, dst.at[fa - d], w_s.at[d - 1, i], w_r.at[fa - d - 1, i], y_peer(d)
            )

    late = []

    def tok_z(s):
        for j in range(1, chips):
            to = (z_at + j) % chips

            copy = remote(
                tok.at[s, mine], tok.at[s, mine], tokz_s.at[s, j - 1], tokz_r.at[s, z_at], z_peer(to)
            )
            direct = distance(to, z_at) != 2

            @pl.when(direct)
            def _(copy=copy):
                copy.start()

            late.append((direct, copy))
        send(remote(tok.at[s, mine], tok.at[s, mine], tokc_s.at[s, z_at], tokc_r.at[s, z_at], core_peer))

    def tok_arrived(s, source):
        at = token_rows(source, c_at)
        remote(tok.at[s, at], tok.at[s, at], tokz_s.at[s, 0], tokz_r.at[s, source], z_peer(z_at)).wait_recv()

    def to_core(s, source):
        at = token_rows(source, c_at)
        send(remote(tok.at[s, at], tok.at[s, at], tokc_s.at[s, source], tokc_r.at[s, source], core_peer))

    def tok_relay(s):
        for side, step in enumerate((1, -1)):
            source, target = z_at - step, z_at + step
            exists = jnp.logical_and(source >= 0, source < chips)
            both = jnp.logical_and(exists, jnp.logical_and(target >= 0, target < chips))
            source = (source + chips) % chips
            target = (target + chips) % chips
            at = token_rows(source, c_at)
            copy = remote(
                tok.at[s, at], tok.at[s, at], relay_s.at[s, side], tokz_r.at[s, source], z_peer(target)
            )

            @pl.when(exists)
            def _(source=source):
                tok_arrived(s, source)

            @pl.when(both)
            def _(copy=copy):
                copy.start()

            late.append((both, copy))

            forward = remote(
                tok.at[s, at], tok.at[s, at], tokc_s.at[s, source], tokc_r.at[s, source], core_peer
            )

            @pl.when(exists)
            def _(forward=forward):
                forward.start()

            late.append((exists, forward))

    def tok_rest(s):
        for j in range(1, chips):
            source = (z_at + j) % chips
            far = distance(source, z_at) > 1
            at = token_rows(source, c_at)
            forward = remote(
                tok.at[s, at], tok.at[s, at], tokc_s.at[s, source], tokc_r.at[s, source], core_peer
            )

            @pl.when(far)
            def _(source=source, forward=forward):
                tok_arrived(s, source)
                forward.start()

            late.append((far, forward))

    def tok_from_core(s):
        for z in range(chips):
            at = token_rows(z, CORES - 1 - c_at)
            remote(tok.at[s, at], tok.at[s, at], tokc_s.at[s, z], tokc_r.at[s, z], core_peer).wait_recv()

    def lanes(j):
        return pl.ds(pl.multiple_of(((z_at + shifts[j]) % chips) * piece, piece), piece)

    def back_slice(slot, step):
        lo, hi, j = steps[step]
        first = 2 * chunks[lo][0]
        last = 2 * (chunks[hi - 1][0] + chunks[hi - 1][1])
        if j is None:
            return back.at[slot, pl.ds(first, last - first)]
        return back.at[slot, pl.ds(first, last - first), lanes(j)]


    def send_back(step):
        for d in range(1, fb):
            copy = remote(
                back_slice(0, step), back_slice(fb - d, step),
                back_s.at[d - 1], back_r.at[fb - d - 1, step], x_peer(d),
            )
            copy.start()

    got = [0]

    def await_back(until):
        while got[0] < until:
            step = got[0]
            for s in range(1, fb):
                remote(
                    back_slice(0, step), back_slice(s, step),
                    back_s.at[0], back_r.at[s - 1, step], x_peer(1 % fb),
                ).wait_recv()
            got[0] += 1

    if tapbuf.shape[0] > hidden:
        tapbuf[hidden:, :] = jnp.zeros((tapbuf.shape[0] - hidden, 128), f32)

    for copy in tok_loads:
        copy.wait()
    tok_z(0)
    next_step = 0
    after_conv = {min(1, len(chunks) - 1): [lambda: [tok_x_done(), [tok_z(s) for s in range(1, fb)]]]}

    def tok_x_done():
        for s in range(1, fb):
            for d_a in range(fa):
                tokx[s, d_a].wait_recv()

    relays = list(range(fb))
    for k, (at, size) in enumerate(chunks):
        if k < len(field_loads):
            for copy in field_loads[k]:
                copy.wait()
        group = 16 if size % 16 == 0 else 8
        conv_rows(group, rows, taps, at, 2 * at, size, fg, fv, fh, kern_ref, back, tapbuf)
        while next_step < len(steps) and steps[next_step][1] <= k + 1:
            send_back(next_step)
            next_step += 1
        for action in after_conv.get(k, []):
            action()
        if k == 3:
            tok_relay(relays.pop(0))

    tap_t = tapbuf[...].T
    tapx[fs_at] = tap_t[0 : tapx.shape[1], :]
    for d in range(1, fs_size):
        to = ((fs_at + d) % fs_size, tp_at)
        copy = remote(tapx.at[fs_at], tapx.at[fs_at], tap_s.at[0], tap_r.at[fs_at], to)
        copy.start()

    def transpose_weights(d):
        for at, size in chunks:
            pair = jnp.concatenate((wg[d, pl.ds(at, size), :], wv[d, pl.ds(at, size), :]), axis=0)
            wt[pl.ds(d * block, block), pl.ds(2 * at, 2 * size)] = pair.T

    inner = (((1,), (0,)), ((), ()))
    mblock = min(256, block)

    def rows_of(ref, r, j, d):
        return ref.at[r, j, pl.ds(d * block, block)]

    def core_copy(r, j, d):
        return remote(
            rows_of(psend, r, j, d), rows_of(precv, r, j, d), pc_s.at[0], pc_r.at[r, j, d], core_peer
        )

    started_early = {}

    def partial_early(r, j, depth):
        right = back[r, 0:depth, lanes(j)]

        def one(i, carry):
            at = pl.ds(pl.multiple_of(i * mblock, mblock), mblock)
            acc[r - 1, at, :] = lax.dot_general(wt[at, 0:depth], right, inner, preferred_element_type=f32)
            return carry

        lax.fori_loop(0, wide // mblock, one, 0)
        started_early[r, j] = depth

    def partial(r, j, d):
        depth = started_early.get((r, j), 0)
        right = back[r, depth:, lanes(j)]

        def one(i, carry):
            at = pl.ds(pl.multiple_of(d * block + i * mblock, mblock), mblock)
            out = lax.dot_general(wt[at, depth:], right, inner, preferred_element_type=f32)
            if depth:
                out = out + acc[r - 1, at, :]
            out = out.astype(bf16)
            own = jnp.where(c_at == 0, out[:, 0:shard], out[:, shard:piece])
            other = jnp.where(c_at == 0, out[:, shard:piece], out[:, 0:shard])
            pown[r, j, at, :] = own
            psend[r, j, at, :] = other
            return carry

        lax.fori_loop(0, block // mblock, one, 0)
        core_copy(r, j, d).start()

    def relay_copy(r, j, d, side, peer):
        return remote(
            rows_of(ssend, r, j, d), relayed.at[r, side, pl.ds(d * block, block)],
            pz_s.at[r, j, d], mid_r.at[r, side, d], peer,
        )

    def chip_copy(r, j, d, peer):
        return remote(
            rows_of(ssend, r, j, d), rows_of(zrecv, r, j, d), pz_s.at[r, j, d], pz_r.at[r, j, d], peer
        )

    def reduce_core(r, j, d):
        core_copy(r, j, d).wait_recv()
        cut = slice(d * block, (d + 1) * block)
        total = pown[r, j, cut].astype(f32) + precv[r, j, cut].astype(f32)
        shift = shifts[j]
        if chips > 2 and shift in (1, chips - 1):
            side = 0 if shift == 1 else 1

            @pl.when(middle)
            def _():
                relay_copy(r, j, d, side, z_peer(z_at)).wait_recv()

            total = total + relayed[r, side, cut].astype(f32)
        ssend[r, j, cut] = total.astype(bf16)
        if shift == 0:
            return
        to = (z_at + shift) % chips
        if not must_be_two(shift):
            direct = distance(to, z_at) != 2
            copy = chip_copy(r, j, d, z_peer(to))
            late.append((direct, copy))

            @pl.when(direct)
            def _():
                copy.start()
        if may_be_two(shift):
            for side, step in enumerate((1, -1)):
                through = to == z_at + 2 * step
                relay = relay_copy(r, j, d, side, z_peer((z_at + step + chips) % chips))
                late.append((through, relay))

                @pl.when(through)
                def _(relay=relay):
                    relay.start()

    def reduce_chips(r, d):
        cut = slice(d * block, (d + 1) * block)
        total = ssend[r, chips - 1, cut].astype(f32)
        for j in range(chips - 1):
            if must_be_two(shifts[j]):
                continue

            @pl.when(distance((z_at + chips - shifts[j]) % chips, z_at) != 2)
            def _(j=j):
                chip_copy(r, j, d, z_peer(z_at)).wait_recv()

            total = total + zrecv[r, j, cut].astype(f32)
        return total.astype(bf16).T

    saves = []

    def save(src, dst):
        copy = pltpu.make_async_copy(src, dst, save_sem.at[len(saves)])
        copy.start()
        saves.append(copy)

    def gradient(k):
        at, size = chunks[k]
        cut = pl.ds(2 * at, 2 * size)
        for d_a in list(range(1, fa)) + [0]:
            cols = slice(d_a * block, (d_a + 1) * block)
            total = lax.dot_general(back[0, cut, :], tok[0, :, cols], inner, preferred_element_type=f32)
            for s in range(1, fb):
                total = total + lax.dot_general(
                    back[s, cut, :], tok[s, :, cols], inner, preferred_element_type=f32
                )
            if d_a:
                gsend[d_a - 1, cut, :] = total.astype(bf16)
                remote(
                    gsend.at[d_a - 1, cut], grecv.at[fa - d_a - 1, cut],
                    g_s.at[d_a - 1], g_r.at[fa - d_a - 1, k], y_peer(d_a),
                ).start()
            else:
                gate_out[pl.ds(at, size), :] = total[:size]
                val_out[pl.ds(at, size), :] = total[size:]

    def finish_gradient(k, norms):
        at, size = chunks[k]
        cut = pl.ds(2 * at, 2 * size)
        for s in range(1, fa):
            remote(
                gsend.at[s - 1, cut], grecv.at[s - 1, cut], g_s.at[s - 1], g_r.at[s - 1, k], y_peer(1 % fa)
            ).wait_recv()
        new = []
        for i, out in enumerate((gate_out, val_out)):
            rows_at = pl.ds(at, size)
            total = out[rows_at, :]
            for s in range(1, fa):
                total = total + grecv[s - 1, pl.ds(2 * at + i * size, size), :].astype(f32)
            out[rows_at, :] = total
            new.append(norms[i] + jnp.sum(total * total, axis=0, keepdims=True))
        if k in (len(chunks) - 4, len(chunks) - 1):
            low = 0 if k == len(chunks) - 4 or len(chunks) < 4 else chunks[len(chunks) - 3][0]
            whole = pl.ds(low, at + size - low)
            save(gate_out.at[whole], gate_done.at[whole])
            save(val_out.at[whole], val_done.at[whole])
        return new

    transpose_weights(0)
    for j in range(chips):
        partial(0, j, 0)
        if j == min(1, chips - 1):
            while relays:
                tok_relay(relays.pop(0))
    for d in range(1, fa):
        for i in range(2):
            w_waits[d, i].wait_recv()
        transpose_weights(d)
        for j in range(chips):
            partial(0, j, d)
            if d == 1 and j == 0:
                reduce_core(0, 0, 0)
            if j == min(1, chips - 1):
                reduce_core(0, 0, d)
    for s in range(fb):
        tok_rest(s)
    for j in range(1, chips):
        for d in range(fa):
            reduce_core(0, j, d)
    for s in range(fb):
        tok_from_core(s)

    def place(slot, d_a, value):
        start = (((a_at + d_a) % fa) * fb + (b_at + slot) % fb) * block
        cut = pl.ds(pl.multiple_of(start, block), block)
        dx_ref[slot, :, d_a * block : (d_a + 1) * block] = value
        save(dx_ref.at[slot, :, pl.ds(d_a * block, block)], dx_out.at[:, cut])

    norms = [jnp.zeros((1, block), f32), jnp.zeros((1, block), f32)]
    waiting, finished = [], 0

    for kind, index, until in ready:
        await_back(until)
        if kind == "chunk":
            gradient(index)
            if chips > 1 and index == len(chunks) - 3 and steps[until][2] == chips - 2:
                for r in range(1, fb):
                    partial_early(r, chips - 2, 2 * chunks[index + 1][0])
            for item in waiting:
                reduce_core(*item)
            waiting = []
            if finished <= index - 3 and until < len(steps) - 2:
                norms = finish_gradient(finished, norms)
                finished += 1
        else:
            for item in waiting:
                reduce_core(*item)
            waiting = []
            for r in range(1, fb):
                for d in range(fa):
                    partial(r, index, d)
                    waiting.append((r, index, d))
            if index == chips - 2:
                for item in waiting:
                    reduce_core(*item)
                waiting = []
    for d in range(fa):
        place(0, d, reduce_chips(0, d))
    for r in range(1, fb):
        for d in range(fa):
            for item in waiting:
                if item[0] == r and item[2] == d:
                    reduce_core(*item)
            cut = pl.ds(d * block, block)
            xsend[r - 1, :, cut] = reduce_chips(r, d)
            send(remote(
                xsend.at[r - 1, :, cut], xrecv.at[fb - r - 1, :, cut],
                out_s.at[r - 1, d], out_r.at[fb - r - 1, d], x_peer(r),
            ))

    tap_total = None
    for f in range(fs_size):
        @pl.when(fs_at != f)
        def _(f=f):
            remote(tapx.at[f], tapx.at[f], tap_s.at[0], tap_r.at[f], (fs_at, tp_at)).wait_recv()

        tap_total = tapx[f] if f == 0 else tap_total + tapx[f]
    tap_held[...] = tap_total
    save(tap_held, tap_out)
    tap_norms = jnp.sum(tap_total * tap_total, axis=1, keepdims=True)
    normx[tp_at, 2 : 2 + 2 * taps, :] = jnp.broadcast_to(tap_norms[0 : 2 * taps], (2 * taps, block))

    for k in range(finished, len(chunks)):
        norms = finish_gradient(k, norms)
    normx[tp_at, 0:1, :] = norms[0]
    normx[tp_at, 1:2, :] = norms[1]
    for d in range(1, tp_size):
        to = (fs_at, (tp_at + d) % tp_size)
        remote(normx.at[tp_at], normx.at[tp_at], norm_s.at[0], norm_r.at[tp_at], to).start()

    for s in range(1, fb):
        for d in range(fa):
            cut = pl.ds(d * block, block)
            remote(
                xsend.at[s - 1, :, cut], xrecv.at[s - 1, :, cut],
                out_s.at[s - 1, d], out_r.at[s - 1, d], x_peer(1 % fb),
            ).wait_recv()
            start = (((a_at + d) % fa) * fb + (b_at + s) % fb) * block
            save(xrecv.at[s - 1, :, cut], dx_out.at[:, pl.ds(pl.multiple_of(start, block), block)])

    norm_total = None
    for t in range(tp_size):
        @pl.when(tp_at != t)
        def _(t=t):
            remote(normx.at[t], normx.at[t], norm_s.at[0], norm_r.at[t], (fs_at, tp_at)).wait_recv()

        norm_total = normx[t] if t == 0 else norm_total + normx[t]
    norm_held[...] = norm_total
    save(norm_held, norm_out)

    for copy in saves:
        copy.wait()
    for d in range(1, fb):
        remote(back.at[0], back.at[fb - d], back_s.at[d - 1], back_r.at[fb - d - 1, 0], x_peer(d)).wait_send()
    for d in range(1, fa):
        remote(
            gsend.at[d - 1], grecv.at[fa - d - 1], g_s.at[d - 1], g_r.at[fa - d - 1, 0], y_peer(d)
        ).wait_send()
    remote(psend, precv, pc_s.at[0], pc_r.at[0, 0, 0], core_peer).wait_send()
    if fs_size > 1:
        others = tapx.at[pl.ds(0, fs_size - 1)]
        remote(others, others, tap_s.at[0], tap_r.at[0], x_peer(1 % fb)).wait_send()
    others = normx.at[pl.ds(0, tp_size - 1)]
    remote(others, others, norm_s.at[0], norm_r.at[0], core_peer).wait_send()
    for copy in sends:
        copy.wait_send()
    for started, copy in late:
        @pl.when(started)
        def _(copy=copy):
            copy.wait_send()


def whole_step(fa, fb, chips, taps, tokens, up_gate, up_val, gate_weight, val_weight, gate_taps, val_taps, hidden_grad):
    f32, bf16 = jnp.float32, jnp.bfloat16
    hidden, rows = up_gate.shape
    shard, width = tokens.shape
    block = gate_weight.shape[1]
    wide = fa * block
    fs_size, tp_size = fa * fb, chips * CORES
    chunks = hidden_chunks(hidden)
    n = len(chunks)
    steps, _ = stream_steps(n, chips)
    padded = -(-hidden // 128) * 128
    tap_rows = -(-2 * taps // 8) * 8
    norm_rows = -(-(2 + 2 * taps) // 8) * 8
    dma = pltpu.SemaphoreType.DMA
    xs, ys = max(1, fb - 1), max(1, fa - 1)
    scratch = [
        pltpu.VMEM((hidden, rows), bf16),
        pltpu.VMEM((hidden, rows), bf16),
        pltpu.VMEM((hidden, rows), bf16),
        pltpu.VMEM((fb, rows, wide), bf16),
        pltpu.VMEM((fb, 2 * hidden, rows), bf16),
        pltpu.VMEM((fa, hidden, block), bf16),
        pltpu.VMEM((fa, hidden, block), bf16),
        pltpu.VMEM((wide, 2 * hidden), bf16),
        pltpu.VMEM((fb, chips, wide, shard), bf16),
        pltpu.VMEM((fb, chips, wide, shard), bf16),
        pltpu.VMEM((fb, chips, wide, shard), bf16),
        pltpu.VMEM((fb, chips, wide, shard), bf16),
        pltpu.VMEM((fb, chips, wide, shard), bf16),
        pltpu.VMEM((xs, shard, wide), bf16),
        pltpu.VMEM((xs, shard, wide), bf16),
        pltpu.VMEM((ys, 2 * hidden, block), bf16),
        pltpu.VMEM((ys, 2 * hidden, block), bf16),
        pltpu.VMEM((padded, 128), f32),
        pltpu.VMEM((fs_size, tap_rows, padded), f32),
        pltpu.VMEM((tp_size, norm_rows, block), f32),
        pltpu.VMEM((fb, 2, wide, shard), bf16),
        pltpu.VMEM((taps, hidden), bf16),
        pltpu.VMEM((taps, hidden), bf16),
        pltpu.VMEM((128, padded), f32),
        pltpu.VMEM((padded, 128), f32),
        pltpu.VMEM((1, shard, wide), bf16),
        pltpu.VMEM((hidden, block), f32),
        pltpu.VMEM((hidden, block), f32),
        pltpu.VMEM((shard, width), bf16),
        pltpu.VMEM((tap_rows, padded), f32),
        pltpu.VMEM((norm_rows, block), f32),
        pltpu.VMEM((xs, wide, CORES * shard), f32),
        dma((fa + 11,)),
        dma((xs, fa)),
        dma((xs, fa)),
        dma((fb, max(1, chips - 1))),
        dma((fb, chips)),
        dma((fb, 2)),
        dma((fb, chips)),
        dma((fb, chips)),
        dma((ys, 2)),
        dma((ys, 2)),
        dma((xs,)),
        dma((xs, len(steps))),
        dma((1,)),
        dma((fb, chips, fa)),
        dma((fb, max(1, chips - 1), fa)),
        dma((fb, max(1, chips - 1), fa)),
        dma((fb, 2, fa)),
        dma((xs, fa)),
        dma((xs, fa)),
        dma((ys,)),
        dma((ys, n)),
        dma((1,)),
        dma((fs_size,)),
        dma((1,)),
        dma((tp_size,)),
        dma((fs_size + 6,)),
    ]
    return pl.pallas_call(
        functools.partial(step_kernel, fa, fb, chips, taps),
        in_specs=[HBM] * 8,
        out_specs=[ANY] * 5,
        out_shape=[
            jax.ShapeDtypeStruct((shard, width), bf16),
            jax.ShapeDtypeStruct((hidden, block), f32),
            jax.ShapeDtypeStruct((hidden, block), f32),
            jax.ShapeDtypeStruct((tap_rows, padded), f32),
            jax.ShapeDtypeStruct((norm_rows, block), f32),
        ],
        scratch_shapes=scratch,
        compiler_params=pltpu.CompilerParams(
            collective_id=0, has_side_effects=True, vmem_limit_bytes=VMEM_LIMIT
        ),
    )(tokens, up_gate, up_val, gate_weight, val_weight, gate_taps, val_taps, hidden_grad)


def results_kernel(
    taps, hidden, dx_in, gate_in, val_in, tap_in, norm_in,
    dx_out, gate_out, val_out, gate_tap, val_tap, gate_norm, val_norm, tap_norm,
    dx, gate, val, tap, norm, gate_tap_held, val_tap_held, gate_norm_held, val_norm_held, tap_norm_held,
    in_sem, out_sem,
):
    half = hidden // 16 * 8
    parts = [(tap_in, tap, None), (norm_in, norm, None)]
    for cut in (pl.ds(0, half), pl.ds(half, hidden - half)):
        for src, held, dst in ((gate_in, gate, gate_out), (val_in, val, val_out)):
            parts.append((src.at[cut], held.at[cut], dst.at[cut]))
    parts.append((dx_in, dx, dx_out))
    ins = [pltpu.make_async_copy(src, held, in_sem.at[i]) for i, (src, held, _) in enumerate(parts)]
    for copy in ins:
        copy.start()
    outs = []

    def out(held, dst):
        outs.append(pltpu.make_async_copy(held, dst, out_sem.at[len(outs)]))
        outs[-1].start()

    ins[0].wait()
    gate_tap_held[...] = tap[0:taps, 0:hidden]
    val_tap_held[...] = tap[taps : 2 * taps, 0:hidden]
    ins[1].wait()
    gate_norm_held[...] = norm[0, :]
    val_norm_held[...] = norm[1, :]
    for i in range(2):
        for t in range(taps):
            tap_norm_held[i : i + 1, t : t + 1] = norm[2 + i * taps + t : 3 + i * taps + t, 0:1]
    for held, dst in (
        (gate_tap_held, gate_tap), (val_tap_held, val_tap), (gate_norm_held, gate_norm),
        (val_norm_held, val_norm), (tap_norm_held, tap_norm),
    ):
        out(held, dst)
    for i, (_, held, dst) in enumerate(parts):
        if dst is not None:
            ins[i].wait()
        if dst is not None:
            out(held, dst)
    for copy in outs:
        copy.wait()


def results(taps, hidden, dx, gate, val, tap, norm):
    f32 = jnp.float32
    block = norm.shape[1]
    small = [((taps, hidden), f32)] * 2 + [((block,), f32)] * 2 + [((2, taps), f32)]
    return pl.pallas_call(
        functools.partial(results_kernel, taps, hidden),
        in_specs=[ANY] * 5,
        out_specs=[ANY] * 8,
        out_shape=[jax.ShapeDtypeStruct(v.shape, v.dtype) for v in (dx, gate, val)]
        + [jax.ShapeDtypeStruct(*kind) for kind in small],
        scratch_shapes=[pltpu.VMEM(v.shape, v.dtype) for v in (dx, gate, val, tap, norm)]
        + [pltpu.VMEM(*kind) for kind in small]
        + [pltpu.SemaphoreType.DMA((7,)), pltpu.SemaphoreType.DMA((10,))],
        compiler_params=pltpu.CompilerParams(vmem_limit_bytes=VMEM_LIMIT),
    )(dx, gate, val, tap, norm)


def solution(mesh):
    fs_size, tp_size = mesh.shape["fs"], mesh.shape["tp"]
    fb = max(d for d in range(1, fs_size + 1) if fs_size % d == 0 and d * d <= fs_size)
    fa = fs_size // fb
    chips = tp_size // CORES

    def local(tokens, up_gate, up_val, gate_weight, val_weight, gate_taps, val_taps, hidden_grad):
        taps, hidden = gate_taps.shape
        dx, gate_grad, val_grad, tap_grad, norms = whole_step(
            fa, fb, chips, taps, tokens, up_gate.T, up_val.T, gate_weight.T, val_weight.T,
            gate_taps, val_taps, hidden_grad.T,
        )
        dx, gate_grad, val_grad, gate_tap, val_tap, gate_norm, val_norm, tap_norm = results(
            taps, hidden, dx, gate_grad, val_grad, tap_grad, norms
        )
        return dx, gate_grad.T, val_grad.T, gate_tap, val_tap, gate_norm, val_norm, tap_norm

    in_specs = (
        P(("fs", "tp"), None),
        P("fs", "tp"),
        P("fs", "tp"),
        P("fs", "tp"),
        P("fs", "tp"),
        P(None, "tp"),
        P(None, "tp"),
        P("fs", "tp"),
    )
    out_specs = (
        P(("fs", "tp"), None),
        P("fs", "tp"),
        P("fs", "tp"),
        P(None, "tp"),
        P(None, "tp"),
        P("fs"),
        P("fs"),
        P(),
    )
    return jax.shard_map(local, mesh=mesh, in_specs=in_specs, out_specs=out_specs, check_vma=False)
```
